256 devices in a mesh: sp: 16 (over y, x), dp: 16 (over z, core).
Axes of the slice: x: 4, y: 4, z: 8, core: 2. Of those that a mesh axis runs over, the one named last changes fastest.
Arguments:
- tokens: bfloat16 [16, 6144, 2048], P('dp', 'sp'), may hold values from -6 to 6
- value_act: bfloat16 [16, 6144, 1024], P('dp', 'sp'), may hold values from -6 to 6
- gate_act: bfloat16 [16, 6144, 1024], P('dp', 'sp'), may hold values from -6 to 6
- cotangent: bfloat16 [16, 6144, 1024], P('dp', 'sp'), may hold values from -6 to 6
- value_weight: bfloat16 [2048, 1024], P('dp'), may hold values from -0.1875 to 0.1875
- gate_weight: bfloat16 [2048, 1024], P('dp'), may hold values from -0.1875 to 0.1875
- norm_gain: float32 [1024], replicated, may hold values from 0.1 to 1.9
- norm_bias: float32 [1024], replicated, may hold values from -3 to 3
- mix_weight: bfloat16 [16, 128, 128], replicated, may hold values from -0.5 to 0.5
- mix_bias: float32 [16, 128], replicated, may hold values from 0.1 to 1.9
Outputs:
- tokens_grad: bfloat16 [16, 6144, 2048], P('dp', 'sp')
- value_weight_grad: float32 [2048, 1024], P('dp')
- gate_weight_grad: float32 [2048, 1024], P('dp')
- mix_weight_grad: float32 [16, 128, 128], replicated
- mix_bias_grad: float32 [16, 128], replicated
- norm_gain_grad: float32 [1024], replicated
- norm_bias_grad: float32 [1024], replicated
The draws below stay inside these ranges and needn't reach their ends.
All inputs are finite; a program needn't handle non-finite values.
Results may differ from the reference program's by a relative error of at most 0.0054.
Values may be sent and summed in bfloat16 or wider, within the bound.
A program may use at most 128 MiB of HBM per device.

```python
import jax
import jax.numpy as jnp
from jax import lax

D = 2048
GROUPS = 16
DG = 1024
BLOCK = 128
SEQ = 6144
SEQS = 16


def strengthened(array, stream_key, source, target, parts, factor):
    owner, partner = [(jnp.arange(array.shape[dim]) // (array.shape[dim] // parts)).reshape([-1 if axis == dim else 1 for axis in range(array.ndim)]) for dim in (source, target)]
    chosen = jax.random.permutation(stream_key, parts)[partner]
    strong = (owner == chosen) | (owner == (partner + parts // 2) % parts)
    return jnp.where(strong, factor * array, array)


def block_scale(rng, shape, split, least, high):
    level, own = 1.0, jax.random.fold_in(rng, 6)
    for axis_at, parts in split:
        steps = jnp.exp(jax.random.uniform(jax.random.fold_in(own, axis_at), (parts,), jnp.float32, least / len(split), high / len(split)))
        level = level * jnp.repeat(steps, shape[axis_at] // parts).reshape([-1 if axis == axis_at else 1 for axis in range(len(shape))])
    return level


def scatter_about(stream_key, dims, scale, bound, split=(), kind=jnp.bfloat16):
    loudness = block_scale(stream_key, dims, split, -0.22, 0.18) if split else 1.0
    values = jax.random.normal(stream_key, dims, jnp.float32) * scale * loudness
    return jnp.minimum(jnp.maximum(values, -bound), bound).astype(kind)


def noise_with(stream_key, dims, spread, most, shards, heavy, kind=jnp.bfloat16):
    array = spread * jax.random.normal(stream_key, dims, jnp.float32)
    if shards:
        array = array * block_scale(stream_key, dims, shards, -0.22, 0.18)
    return jnp.clip(strengthened(array, jax.random.fold_in(stream_key, 3), *heavy), -most, most).astype(kind)


def setup_inputs(seed: int = 0) -> dict:
    key_of = jax.random.split(jax.random.key(seed), 11)
    tokens = noise_with(key_of[0], (SEQS, SEQ, D), 1.0, 6.0, ((0, 16), (1, 16)), (1, 2, 16, 2.0))
    value_act = scatter_about(key_of[1], (SEQS, SEQ, DG), 1.0, 6.0, ((0, 16), (1, 16)))
    gate_act = scatter_about(key_of[2], (SEQS, SEQ, DG), 1.0, 6.0, ((0, 16), (1, 16)))
    cotangent = scatter_about(key_of[3], (SEQS, SEQ, DG), 1.0, 6.0, ((0, 16), (1, 16)))
    value_weight = scatter_about(key_of[4], (D, DG), DG ** -0.5, 0.1875, ((0, 16),))
    gate_weight = scatter_about(key_of[5], (D, DG), DG ** -0.5, 0.1875, ((0, 16),))
    norm_gain = jnp.clip(1.0 + 0.18 * jax.random.normal(key_of[6], (DG,), jnp.float32), 0.1, 1.9)
    norm_bias = scatter_about(key_of[7], (DG,), 0.5, 3.0, (), jnp.float32)
    mix_weight = scatter_about(key_of[8], (GROUPS, BLOCK, BLOCK), BLOCK ** -0.5, 0.5)
    mix_bias = jnp.clip(1.0 + 0.18 * jax.random.normal(key_of[9], (GROUPS, BLOCK), jnp.float32), 0.1, 1.9)
    return {"tokens": tokens, "value_act": value_act, "gate_act": gate_act, "cotangent": cotangent, "value_weight": value_weight, "gate_weight": gate_weight, "norm_gain": norm_gain, "norm_bias": norm_bias, "mix_weight": mix_weight, "mix_bias": mix_bias}


EPSILON = 1e-06

def gelu_slope(values):
    cdf_part = 0.5 * (1.0 + lax.erf(values * 0.7071067811865476))
    pdf_part = jnp.exp(-0.5 * values * values) * 0.3989422804014327
    return cdf_part + values * pdf_part

def mixer_backward(value_act, gate_act, cotangent, norm_gain, norm_bias, mix_weight, mix_bias):
    seq_len, channels = value_act.shape
    groups, block_len = (mix_weight.shape[0], mix_weight.shape[1])
    group_dim = channels // groups
    blocks = seq_len // block_len
    value_float = value_act.astype(jnp.float32)
    gate_float = gate_act.astype(jnp.float32)
    activated = jax.nn.gelu(value_float, approximate=False)
    gate_gelu = jax.nn.gelu(gate_float, approximate=False)
    centred = gate_gelu - lax.optimization_barrier(jnp.mean(gate_gelu, axis=-1, keepdims=True))
    inv_std = lax.rsqrt(lax.optimization_barrier(jnp.mean(centred * centred, axis=-1, keepdims=True)) + EPSILON)
    normed = centred * inv_std
    spread_in = (normed * norm_gain + norm_bias).astype(jnp.bfloat16)
    spread_in = spread_in.reshape(blocks, block_len, groups, group_dim)
    causal = jnp.tril(jnp.ones((block_len, block_len), dtype=bool))
    masked_weight = jnp.where(causal[None], mix_weight, jnp.zeros_like(mix_weight))
    spatial = jnp.einsum('gts,bsgd->btgd', masked_weight.astype(jnp.float32), spread_in.astype(jnp.float32))
    spatial = (spatial + mix_bias.T[None, :, :, None]).reshape(seq_len, channels)
    grad_out = cotangent.astype(jnp.float32)
    grad_act = grad_out * spatial
    grad_spatial = grad_out * activated
    grad_split = grad_spatial.reshape(blocks, block_len, groups, group_dim)
    bias_grad = lax.optimization_barrier(jnp.sum(grad_split, axis=(0, 3))).T
    spatial_low = grad_split.astype(jnp.bfloat16)
    weight_grad = jnp.einsum('btgd,bsgd->gts', spatial_low.astype(jnp.float32), spread_in.astype(jnp.float32))
    weight_grad = jnp.where(causal[None], weight_grad, jnp.zeros_like(weight_grad))
    grad_norm = jnp.einsum('gts,btgd->bsgd', masked_weight.astype(jnp.float32), spatial_low.astype(jnp.float32))
    grad_norm = grad_norm.reshape(seq_len, channels)
    gain_grad = lax.optimization_barrier(jnp.sum(grad_norm * normed, axis=0))
    shift_grad = lax.optimization_barrier(jnp.sum(grad_norm, axis=0))
    grad_hat = grad_norm * norm_gain
    grad_gate = inv_std * (grad_hat - lax.optimization_barrier(jnp.mean(grad_hat, axis=-1, keepdims=True)) - normed * lax.optimization_barrier(jnp.mean(grad_hat * normed, axis=-1, keepdims=True)))
    value_grad = (grad_act * gelu_slope(value_float)).astype(jnp.bfloat16)
    gate_grad = (grad_gate * gelu_slope(gate_float)).astype(jnp.bfloat16)
    return (value_grad, gate_grad, (weight_grad, bias_grad, gain_grad, shift_grad))

def reference(tokens, value_act, gate_act, cotangent, value_weight, gate_weight, norm_gain, norm_bias, mix_weight, mix_bias):
    both_weights = jnp.concatenate((value_weight, gate_weight), axis=1)

    def per_sequence(running, seq_items):
        inputs, value_seq, gate_seq, cot_seq = seq_items
        value_grad, gate_grad, stats = mixer_backward(value_seq, gate_seq, cot_seq, norm_gain, norm_bias, mix_weight, mix_bias)
        both_grads = jnp.concatenate((value_grad, gate_grad), axis=1)
        input_grad = jnp.dot(both_grads, both_weights.T, preferred_element_type=jnp.float32).astype(jnp.bfloat16)
        weight_sums = running[0] + jnp.dot(inputs.T, both_grads, preferred_element_type=jnp.float32)
        updated = (weight_sums,) + tuple((old + term for old, term in zip(running[1:], stats)))
        return (updated, input_grad)
    initial = (jnp.zeros((D, 2 * DG), jnp.float32), jnp.zeros((GROUPS, BLOCK, BLOCK), jnp.float32), jnp.zeros((GROUPS, BLOCK), jnp.float32), jnp.zeros((DG,), jnp.float32), jnp.zeros((DG,), jnp.float32))
    running, input_grads = lax.scan(per_sequence, initial, (tokens, value_act, gate_act, cotangent))
    return (input_grads, running[0][:, :DG], running[0][:, DG:], running[1], running[2], running[3], running[4])
```

```python
import functools
import jax
import jax.numpy as jnp
from jax import lax
from jax.experimental import pallas as pl
from jax.experimental.pallas import tpu as pltpu
from jax.sharding import PartitionSpec as P

EPSILON = 1e-06
F32, BF16 = jnp.float32, jnp.bfloat16
NT = (((1,), (1,)), ((), ()))
TN = (((0,), (0,)), ((), ()))
NN = (((1,), (0,)), ((), ()))


def dot(a, b, dims=NN):
    return lax.dot_general(a, b, dims, preferred_element_type=F32)


def split3(v):
    hi = v.astype(BF16)
    rest = v - hi.astype(F32)
    mid = rest.astype(BF16)
    low = (rest - mid.astype(F32)).astype(BF16)
    return hi, mid, low


def phi_terms(v):
    cdf = 0.5 * (1.0 + lax.erf(v * 0.7071067811865476))
    pdf = jnp.exp(-0.5 * v * v) * 0.3989422804014327
    return cdf, cdf + v * pdf


def mixer(va, ga, cot, gain, bias, mixw, mixb, grads, wgrad, stats,
          mcat, mtrn, normed, slope, spread, low, cv, gnorm, inv, gsum, bfull, acc_g, acc_b):
    rows = 16
    row = lax.broadcasted_iota(jnp.int32, (128, 128), 0)
    col = lax.broadcasted_iota(jnp.int32, (128, 128), 1)
    keep = row >= col

    def prep(p, _):
        for h in range(2):
            m = jnp.where(keep, mixw[2 * p + h].astype(F32), 0.0)
            mcat[p, :, h * 128:(h + 1) * 128] = m.astype(BF16)
            mtrn[p, :, h * 128:(h + 1) * 128] = m.T.astype(BF16)
        return 0

    lax.fori_loop(0, 8, prep, 0)
    group = lax.broadcasted_iota(jnp.int32, (16, 1024), 0)
    chan = lax.broadcasted_iota(jnp.int32, (16, 1024), 1) // 64
    pick = jnp.where(group == chan, 1.0, 0.0).astype(BF16)
    parts = split3(mixb[...])
    bfull[...] = dot(parts[0], pick, TN) + dot(parts[1], pick, TN) + dot(parts[2], pick, TN)
    gsum[...] = jnp.zeros_like(gsum)
    acc_g[...] = jnp.zeros_like(acc_g)
    acc_b[...] = jnp.zeros_like(acc_b)

    def first(i, _):
        at = pl.ds(pl.multiple_of(i * rows, rows), rows)
        v = va[at, :].astype(F32)
        cdf, slp = phi_terms(v)
        c = cot[at, :].astype(F32)
        gs = c * (v * cdf)
        low[at, :] = gs.astype(BF16)
        cv[at, :] = c * slp
        inb = pl.ds(pl.multiple_of(lax.rem(i, 8) * rows, rows), rows)
        gsum[inb, :] += gs
        return 0

    lax.fori_loop(0, 24, first, 0)

    def second(i, _):
        at = pl.ds(pl.multiple_of(i * rows, rows), rows)
        v = ga[at, :].astype(F32)
        cdf, slp = phi_terms(v)
        slope[at, :] = slp
        g = v * cdf
        cen = g - jnp.mean(g, axis=-1, keepdims=True)
        s = lax.rsqrt(jnp.mean(cen * cen, axis=-1, keepdims=True) + EPSILON)
        n = cen * s
        normed[at, :] = n
        inv[at, :] = jnp.broadcast_to(s, (rows, 128))
        spread[at, :] = (n * gain[...] + bias[...]).astype(BF16)
        return 0

    lax.fori_loop(0, 24, second, 0)

    lane = lax.broadcasted_iota(jnp.int32, (1, 128), 1)
    m0 = jnp.where(lane < 64, 1.0, 0.0).astype(BF16)
    m1 = jnp.where(lane < 64, 0.0, 1.0).astype(BF16)

    def mix(p, _):
        cols = pl.ds(pl.multiple_of(p * 128, 128), 128)
        wg = None
        for b in range(3):
            r = slice(b * 128, (b + 1) * 128)
            s = spread[r, cols]
            l = low[r, cols]
            stack_s = jnp.concatenate((s * m0, s * m1), axis=0)
            stack_l = jnp.concatenate((l * m0, l * m1), axis=0)
            spatial = dot(mcat[p], stack_s) + bfull[:, cols]
            grads[r, cols] = (cv[r, cols] * spatial).astype(BF16)
            gnorm[r, cols] = dot(mtrn[p], stack_l)
            term = dot(stack_l, s, NT)
            wg = term if wg is None else wg + term
        wgrad[2 * p] = jnp.where(keep, wg[:128], 0.0)
        wgrad[2 * p + 1] = jnp.where(keep, wg[128:], 0.0)
        return 0

    lax.fori_loop(0, 8, mix, 0)

    def last(i, _):
        at = pl.ds(pl.multiple_of(i * rows, rows), rows)
        gn = gnorm[at, :]
        n = normed[at, :]
        gnn = gn * n
        acc_g[...] += gnn
        acc_b[...] += gn
        h = gn * gain[...]
        mean_h = jnp.mean(h, axis=-1, keepdims=True)
        mean_hn = jnp.mean(h * n, axis=-1, keepdims=True)
        s = inv[at, 0:1]
        out = s * (h - mean_h - n * mean_hn)
        grads[at, 1024:2048] = (out * slope[at, :]).astype(BF16)
        return 0

    lax.fori_loop(0, 24, last, 0)
    parts = split3(gsum[...])
    stats[0:16, :] = dot(pick, parts[0], NT) + dot(pick, parts[1], NT) + dot(pick, parts[2], NT)
    tot_g = jnp.sum(acc_g[...], axis=0, keepdims=True)
    tot_b = jnp.sum(acc_b[...], axis=0, keepdims=True)
    for k in range(8):
        stats[16 + k:17 + k, :] = tot_g[:, k * 128:(k + 1) * 128]
        stats[24 + k:25 + k, :] = tot_b[:, k * 128:(k + 1) * 128]


MIXER_SCRATCH = (
    pltpu.VMEM((8, 128, 256), BF16),
    pltpu.VMEM((8, 128, 256), BF16),
    pltpu.VMEM((384, 1024), F32),
    pltpu.VMEM((384, 1024), F32),
    pltpu.VMEM((384, 1024), BF16),
    pltpu.VMEM((384, 1024), BF16),
    pltpu.VMEM((384, 1024), F32),
    pltpu.VMEM((384, 1024), F32),
    pltpu.VMEM((384, 128), F32),
    pltpu.VMEM((128, 1024), F32),
    pltpu.VMEM((128, 1024), F32),
    pltpu.VMEM((16, 1024), F32),
    pltpu.VMEM((16, 1024), F32),
)


def mixer_call(va, ga, cot, gain, bias, mixw, mixb):
    vm = pl.BlockSpec(memory_space=pltpu.VMEM)
    return pl.pallas_call(
        mixer,
        out_shape=(
            jax.ShapeDtypeStruct((384, 2048), BF16),
            jax.ShapeDtypeStruct((16, 128, 128), F32),
            jax.ShapeDtypeStruct((32, 128), F32),
        ),
        in_specs=[vm] * 7,
        out_specs=(vm, vm, vm),
        scratch_shapes=list(MIXER_SCRATCH),
        compiler_params=pltpu.CompilerParams(vmem_limit_bytes=60 * 1024 * 1024),
        name="mixer",
    )(va, ga, cot, gain, bias, mixw, mixb)


def reducer(tokens, grads, vw, gw, wgrad, stats,
            tgrad, vout, gout, mixout, statout,
            tokr, gradr, tt, wbuf,
            sfar, sup, sdn, fup, fdn, own1, agg, rlay, rprev, rnext, s1f, s1b, r2, own2, s2b, r3, fin, allf,
            mrecv, mq, mqb, mr1, mq1, mq1b, mr2, my, maz, max_, macc, mpart, mrp,
            stc, stx, sty, stz, st0,
            tok_s, tok_r, grd_s, grd_r, ring_s, ring_r, pair_s, pair_r, one_s, one_r, two_s, two_r,
            thr_s, thr_r, fou_s, fou_r, mix_s, mix_r, sts_s, sts_r):
    sp = lax.axis_index("sp")
    dp = lax.axis_index("dp")
    y, x = sp // 4, lax.rem(sp, 4)
    z, c = dp // 2, lax.rem(dp, 2)
    pc = 1 - c

    def at(nx=None, ny=None, nz=None, nc=None):
        nx = x if nx is None else nx
        ny = y if ny is None else ny
        nz = z if nz is None else nz
        nc = c if nc is None else nc
        return {"sp": ny * 4 + nx, "dp": nz * 2 + nc}

    def along(axis, k):
        if axis == "x":
            return at(nx=lax.rem(x + k, 4))
        if axis == "y":
            return at(ny=lax.rem(y + k, 4))
        return at(nz=lax.rem(z + k, 8))

    def copy(src, dst, ssem, rsem, to):
        return pltpu.make_async_remote_copy(
            src_ref=src, dst_ref=dst, send_sem=ssem, recv_sem=rsem,
            device_id=to, device_id_type=pl.DeviceIdType.MESH)

    def await_recv(dst, ssem, rsem):
        copy(dst, dst, ssem, rsem, at(nc=pc)).wait_recv()

    def await_send(src, ssem, rsem):
        copy(src, src, ssem, rsem, at(nc=pc)).wait_send()

    barrier = pltpu.get_barrier_semaphore()
    pl.semaphore_signal(barrier, inc=1, device_id=at(nc=pc), device_id_type=pl.DeviceIdType.MESH)
    for k in range(1, 8):
        pl.semaphore_signal(barrier, inc=1, device_id=along("z", k), device_id_type=pl.DeviceIdType.MESH)
    for k in range(1, 16):
        pl.semaphore_signal(barrier, inc=1, device_id={"sp": lax.rem(sp + k, 16), "dp": dp},
                            device_id_type=pl.DeviceIdType.MESH)
    pl.semaphore_wait(barrier, 23)

    for k in range(8):
        lanes = pl.ds(pl.multiple_of((2 * k + pc) * 128, 128), 128)
        copy(tokens.at[:, lanes], tokr.at[k], tok_s.at[0], tok_r.at[0], at(nc=pc)).start()
    for h in range(2):
        copy(grads.at[:, pl.ds(h * 1024, 1024)], gradr.at[h], grd_s.at[h], grd_r.at[h], at(nc=pc)).start()
    shard = (vw, gw)

    def chunk(zz, v, cc):
        return wbuf.at[zz, v, cc]

    def hop(direction, v, h):
        if h == 1:
            src = shard[v]
            origin = z
        else:
            origin = lax.rem(z - (h - 1) + 8, 8) if direction == 0 else lax.rem(z + (h - 1), 8)
            src = chunk(origin, v, c)
        i = (direction * 2 + v) * 4 + h - 1
        return copy(src, chunk(origin, v, c), ring_s.at[i], ring_r.at[i], along("z", 1 if direction == 0 else 7))

    def last_hop(direction, v):
        return 4 if direction == v else 3

    for v in range(2):
        for direction in range(2):
            hop(direction, v, 1).start()
    for v in range(2):
        copy(shard[v], chunk(z, v, c), pair_s.at[v], pair_r.at[v], at(nc=pc)).start()
        wbuf[z, v, c] = shard[v][...]
    for k in range(8):
        copy(wgrad.at[2 * k + pc], mrecv.at[k], mix_s.at[0], mix_r.at[0], at(nc=pc)).start()
    copy(stats, stc, sts_s.at[0], sts_r.at[0], at(nc=pc)).start()

    def ring_step(h):
        for v in range(2):
            for direction in range(2):
                if h > last_hop(direction, v):
                    continue
                hop(direction, v, h).wait_recv()
                if h < last_hop(direction, v):
                    hop(direction, v, h + 1).start()
                origin = lax.rem(z - h + 8, 8) if direction == 0 else lax.rem(z + h, 8)
                i = 2 + (direction * 2 + v) * 4 + h - 1
                copy(chunk(origin, v, c), chunk(origin, v, c), pair_s.at[i], pair_r.at[i], at(nc=pc)).start()

    def await_pair(h):
        for v in range(2):
            if h == 0:
                await_recv(chunk(0, v, 0), pair_s.at[v], pair_r.at[v])
                continue
            for direction in range(2):
                if h <= last_hop(direction, v):
                    i = 2 + (direction * 2 + v) * 4 + h - 1
                    await_recv(chunk(0, v, 0), pair_s.at[i], pair_r.at[i])

    def into_tokens(zz):
        wv = wbuf[zz, 0].reshape(256, 1024)
        wg = wbuf[zz, 1].reshape(256, 1024)
        out = dot(grads[:, 0:1024], wv, NT) + dot(grads[:, 1024:2048], wg, NT)
        tgrad[:, pl.ds(pl.multiple_of(zz * 256, 256), 256)] = out.astype(BF16)

    for k in range(8):
        lanes = pl.ds(pl.multiple_of((2 * k + c) * 128, 128), 128)
        tt[k * 128:(k + 1) * 128, 0:384] = tokens[:, lanes].T
    await_recv(tokr, tok_s.at[0], tok_r.at[0])
    for k in range(8):
        tt[k * 128:(k + 1) * 128, 384:768] = tokr[k].T

    def product(h, dest, m):
        lanes = pl.ds(pl.multiple_of(dest * 256, 256), 256)
        wide = pl.ds(pl.multiple_of(h * 1024 + dest * 256, 256), 256)
        rows = pl.ds(pl.multiple_of(m * 256, 256), 256)
        return (dot(tt[rows, 0:384], grads[:, wide]) + dot(tt[rows, 384:768], gradr[h, :, lanes]))

    axes = ("x", "y")
    place = (x, y)
    for h in range(2):
        await_recv(gradr.at[h], grd_s.at[h], grd_r.at[h])
        me = place[h]
        far, up, dn = lax.rem(me + 2, 4), lax.rem(me + 1, 4), lax.rem(me + 3, 4)

        def tile_far(m, _):
            sfar[h, m] = product(h, far, m).astype(BF16)
            return 0

        def tile_up(m, _):
            v = product(h, up, m)
            fup[h, m] = v
            sup[h, m] = v.astype(BF16)
            return 0

        def tile_dn(m, _):
            v = product(h, dn, m)
            fdn[h, m] = v
            sdn[h, m] = v.astype(BF16)
            return 0

        def tile_own(m, _):
            own1[h, m] = product(h, me, m)
            return 0

        o = h * 6
        lax.fori_loop(0, 4, tile_far, 0)
        copy(sfar.at[h, 0:2], rlay.at[h, 0], one_s.at[o], one_r.at[o], along(axes[h], 1)).start()
        copy(sfar.at[h, 2:4], rlay.at[h, 1], one_s.at[o + 1], one_r.at[o + 1], along(axes[h], 3)).start()
        lax.fori_loop(0, 4, tile_up, 0)
        copy(sup.at[h, 2:4], rprev.at[h, 1], one_s.at[o + 2], one_r.at[o + 2], along(axes[h], 1)).start()
        lax.fori_loop(0, 4, tile_dn, 0)
        copy(sdn.at[h, 0:2], rnext.at[h, 0], one_s.at[o + 3], one_r.at[o + 3], along(axes[h], 3)).start()
        lax.fori_loop(0, 4, tile_own, 0)

    await_recv(stc, sts_s.at[0], sts_r.at[0])
    st0[0] = stats[...] + stc[...]
    stx[x] = st0[0]
    for k in range(1, 4):
        copy(st0.at[0], stx.at[x], sts_s.at[1], sts_r.at[1], along("x", k)).start()
    await_recv(mrecv, mix_s.at[0], mix_r.at[0])
    for k in range(8):
        v = wgrad[2 * k + c] + mrecv[k]
        mq[k] = v.reshape(4, 32, 128)
        mqb[k] = v.astype(BF16).reshape(4, 32, 128)
    for k in range(1, 4):
        copy(mqb.at[:, lax.rem(x + k, 4)], mr1.at[k - 1], mix_s.at[1], mix_r.at[1], along("x", k)).start()

    ring_step(1)

    for h in range(2):
        o = h * 6
        await_recv(rlay.at[h, 0], one_s.at[o], one_r.at[o])
        agg[h, 0] = (fup[h, 0:2] + rlay[h, 0].astype(F32)).astype(BF16)
        copy(agg.at[h, 0], rprev.at[h, 0], one_s.at[o + 4], one_r.at[o + 4], along(axes[h], 1)).start()
        await_recv(rlay.at[h, 1], one_s.at[o + 1], one_r.at[o + 1])
        agg[h, 1] = (fdn[h, 2:4] + rlay[h, 1].astype(F32)).astype(BF16)
        copy(agg.at[h, 1], rnext.at[h, 1], one_s.at[o + 5], one_r.at[o + 5], along(axes[h], 3)).start()

    await_recv(stx.at[pl.ds(0, 3)], sts_s.at[1], sts_r.at[1])
    st0[1] = (stx[0] + stx[1]) + (stx[2] + stx[3])
    sty[y] = st0[1]
    for k in range(1, 4):
        copy(st0.at[1], sty.at[y], sts_s.at[2], sts_r.at[2], along("y", k)).start()
    await_recv(mr1, mix_s.at[1], mix_r.at[1])
    v = mq[:, x] + (mr1[0].astype(F32) + mr1[1].astype(F32)) + mr1[2].astype(F32)
    mq1[...] = v
    mq1b[...] = v.astype(BF16)
    for k in range(1, 8):
        copy(mq1b.at[lax.rem(z + k, 8)], mr2.at[k - 1], mix_s.at[2], mix_r.at[2], along("z", k)).start()

    await_pair(0)
    into_tokens(z)
    ring_step(2)

    await_recv(sty.at[pl.ds(0, 3)], sts_s.at[2], sts_r.at[2])
    st0[2] = (sty[0] + sty[1]) + (sty[2] + sty[3])
    stz[z] = st0[2]
    for k in range(1, 8):
        copy(st0.at[2], stz.at[z], sts_s.at[3], sts_r.at[3], along("z", k)).start()
    await_recv(mr2, mix_s.at[2], mix_r.at[2])
    v = mq1[z]
    for k in range(7):
        v = v + mr2[k].astype(F32)
    mpart[...] = v
    my[y] = v
    for k in range(1, 4):
        copy(mpart, my.at[y], mix_s.at[3], mix_r.at[3], along("y", k)).start()

    for h in range(2):
        o = h * 6
        for i, buf in ((2, rprev.at[h, 1]), (4, rprev.at[h, 0]), (3, rnext.at[h, 0]), (5, rnext.at[h, 1])):
            await_recv(buf, one_s.at[o + i], one_r.at[o + i])
        for q in range(4):
            v = own1[h, q] + (rprev[h, q // 2, q % 2].astype(F32) + rnext[h, q // 2, q % 2].astype(F32))
            v = v.reshape(2, 4, 32, 256)
            s1f[h, 2 * q:2 * q + 2] = v
            s1b[h, 2 * q:2 * q + 2] = v.astype(BF16)
        other = place[1 - h]
        for k in range(1, 4):
            copy(s1b.at[h, :, lax.rem(other + k, 4)], r2.at[h, k - 1], two_s.at[h], two_r.at[h],
                 along(axes[1 - h], k)).start()

    await_pair(1)
    into_tokens(lax.rem(z + 1, 8))
    into_tokens(lax.rem(z + 7, 8))
    ring_step(3)

    await_recv(my.at[pl.ds(0, 3)], mix_s.at[3], mix_r.at[3])
    v = ((my[0] + my[1]) + (my[2] + my[3])).astype(BF16)
    macc[...] = v
    maz[z] = v
    for k in range(1, 8):
        copy(macc, maz.at[z], mix_s.at[4], mix_r.at[4], along("z", k)).start()

    for h in range(2):
        await_recv(r2.at[h], two_s.at[h], two_r.at[h])
        v = s1f[h, :, place[1 - h]] + (r2[h, 0].astype(F32) + r2[h, 1].astype(F32)) + r2[h, 2].astype(F32)
        own2[h] = v
        s2b[h] = v.astype(BF16)
        for k in range(1, 8):
            copy(s2b.at[h, lax.rem(z + k, 8)], r3.at[h, k - 1], thr_s.at[h], thr_r.at[h], along("z", k)).start()

    await_pair(2)
    into_tokens(lax.rem(z + 2, 8))
    into_tokens(lax.rem(z + 6, 8))

    await_recv(maz.at[pl.ds(0, 7)], mix_s.at[4], mix_r.at[4])
    max_[x] = maz[...]
    for k in range(1, 4):
        copy(maz, max_.at[x], mix_s.at[5], mix_r.at[5], along("x", k)).start()

    for h in range(2):
        await_recv(r3.at[h], thr_s.at[h], thr_r.at[h])
        v = own2[h, z]
        for k in range(7):
            v = v + r3[h, k].astype(F32)
        fin[h] = v.astype(BF16)
        allf[sp, h] = v.astype(BF16)
    for k in range(1, 16):
        copy(fin, allf.at[sp], fou_s.at[0], fou_r.at[0], {"sp": lax.rem(sp + k, 16), "dp": dp}).start()

    await_pair(3)
    into_tokens(lax.rem(z + 3, 8))
    into_tokens(lax.rem(z + 5, 8))
    await_recv(max_.at[pl.ds(0, 3)], mix_s.at[5], mix_r.at[5])
    copy(max_, mrp, mix_s.at[6], mix_r.at[6], at(nc=pc)).start()

    await_recv(stz.at[pl.ds(0, 7)], sts_s.at[3], sts_r.at[3])
    t = stz[0]
    for k in range(1, 8):
        t = t + stz[k]
    statout[...] = t

    ring_step(4)
    await_recv(mrp, mix_s.at[6], mix_r.at[6])
    for k in range(8):
        mixout[2 * k + c] = max_[:, k].reshape(128, 128).astype(F32)
        mixout[2 * k + pc] = mrp[:, k].reshape(128, 128).astype(F32)
    await_pair(4)
    into_tokens(lax.rem(z + 4, 8))

    await_recv(allf.at[pl.ds(0, 15)], fou_s.at[0], fou_r.at[0])
    for s in range(16):
        a, b = s // 4, s % 4
        vout[a * 32:(a + 1) * 32, b * 256:(b + 1) * 256] = allf[s, 0].astype(F32)
        gout[b * 32:(b + 1) * 32, a * 256:(a + 1) * 256] = allf[s, 1].astype(F32)

    await_send(tokr, tok_s.at[0], tok_r.at[0])
    for h in range(2):
        await_send(gradr.at[h], grd_s.at[h], grd_r.at[h])
        for i in range(6):
            await_send(agg.at[h, 0], one_s.at[h * 6 + i], one_r.at[h * 6 + i])
        await_send(r2.at[h], two_s.at[h], two_r.at[h])
        await_send(r3.at[h], thr_s.at[h], thr_r.at[h])
    await_send(allf.at[pl.ds(0, 15)], fou_s.at[0], fou_r.at[0])
    for i, buf in enumerate((mrecv, mr1, mr2, my.at[pl.ds(0, 3)], maz.at[pl.ds(0, 7)],
                             max_.at[pl.ds(0, 3)], mrp)):
        await_send(buf, mix_s.at[i], mix_r.at[i])
    for i, buf in enumerate((stc, stx.at[pl.ds(0, 3)], sty.at[pl.ds(0, 3)], stz.at[pl.ds(0, 7)])):
        await_send(buf, sts_s.at[i], sts_r.at[i])
    for v in range(2):
        await_send(shard[v], pair_s.at[v], pair_r.at[v])
        for direction in range(2):
            for h in range(1, last_hop(direction, v) + 1):
                i = (direction * 2 + v) * 4 + h - 1
                await_send(shard[v], ring_s.at[i], ring_r.at[i])
                await_send(shard[v], pair_s.at[2 + i], pair_r.at[2 + i])


REDUCER_SCRATCH = (
    pltpu.VMEM((8, 384, 128), BF16),
    pltpu.VMEM((2, 384, 1024), BF16),
    pltpu.VMEM((1024, 768), BF16),
    pltpu.VMEM((8, 2, 2, 128, 1024), BF16),
    pltpu.VMEM((2, 4, 256, 256), BF16),
    pltpu.VMEM((2, 4, 256, 256), BF16),
    pltpu.VMEM((2, 4, 256, 256), BF16),
    pltpu.VMEM((2, 4, 256, 256), F32),
    pltpu.VMEM((2, 4, 256, 256), F32),
    pltpu.VMEM((2, 4, 256, 256), F32),
    pltpu.VMEM((2, 2, 2, 256, 256), BF16),
    pltpu.VMEM((2, 2, 2, 256, 256), BF16),
    pltpu.VMEM((2, 2, 2, 256, 256), BF16),
    pltpu.VMEM((2, 2, 2, 256, 256), BF16),
    pltpu.VMEM((2, 8, 4, 32, 256), F32),
    pltpu.VMEM((2, 8, 4, 32, 256), BF16),
    pltpu.VMEM((2, 3, 8, 32, 256), BF16),
    pltpu.VMEM((2, 8, 32, 256), F32),
    pltpu.VMEM((2, 8, 32, 256), BF16),
    pltpu.VMEM((2, 7, 32, 256), BF16),
    pltpu.VMEM((2, 32, 256), BF16),
    pltpu.VMEM((16, 2, 32, 256), BF16),
    pltpu.VMEM((8, 128, 128), F32),
    pltpu.VMEM((8, 4, 32, 128), F32),
    pltpu.VMEM((8, 4, 32, 128), BF16),
    pltpu.VMEM((3, 8, 32, 128), BF16),
    pltpu.VMEM((8, 32, 128), F32),
    pltpu.VMEM((8, 32, 128), BF16),
    pltpu.VMEM((7, 32, 128), BF16),
    pltpu.VMEM((4, 32, 128), F32),
    pltpu.VMEM((8, 32, 128), BF16),
    pltpu.VMEM((4, 8, 32, 128), BF16),
    pltpu.VMEM((32, 128), BF16),
    pltpu.VMEM((32, 128), F32),
    pltpu.VMEM((4, 8, 32, 128), BF16),
    pltpu.VMEM((32, 128), F32),
    pltpu.VMEM((4, 32, 128), F32),
    pltpu.VMEM((4, 32, 128), F32),
    pltpu.VMEM((8, 32, 128), F32),
    pltpu.VMEM((3, 32, 128), F32),
    pltpu.SemaphoreType.DMA((1,)), pltpu.SemaphoreType.DMA((1,)),
    pltpu.SemaphoreType.DMA((2,)), pltpu.SemaphoreType.DMA((2,)),
    pltpu.SemaphoreType.DMA((16,)), pltpu.SemaphoreType.DMA((16,)),
    pltpu.SemaphoreType.DMA((18,)), pltpu.SemaphoreType.DMA((18,)),
    pltpu.SemaphoreType.DMA((12,)), pltpu.SemaphoreType.DMA((12,)),
    pltpu.SemaphoreType.DMA((2,)), pltpu.SemaphoreType.DMA((2,)),
    pltpu.SemaphoreType.DMA((2,)), pltpu.SemaphoreType.DMA((2,)),
    pltpu.SemaphoreType.DMA((1,)), pltpu.SemaphoreType.DMA((1,)),
    pltpu.SemaphoreType.DMA((7,)), pltpu.SemaphoreType.DMA((7,)),
    pltpu.SemaphoreType.DMA((4,)), pltpu.SemaphoreType.DMA((4,)),
)


def reducer_call(tokens, grads, vw, gw, wgrad, stats):
    vm = pl.BlockSpec(memory_space=pltpu.VMEM)
    return pl.pallas_call(
        reducer,
        out_shape=(
            jax.ShapeDtypeStruct((384, 2048), BF16),
            jax.ShapeDtypeStruct((128, 1024), F32),
            jax.ShapeDtypeStruct((128, 1024), F32),
            jax.ShapeDtypeStruct((16, 128, 128), F32),
            jax.ShapeDtypeStruct((32, 128), F32),
        ),
        in_specs=[vm] * 6,
        out_specs=(vm,) * 5,
        scratch_shapes=list(REDUCER_SCRATCH),
        compiler_params=pltpu.CompilerParams(
            collective_id=0, has_side_effects=True, vmem_limit_bytes=62 * 1024 * 1024),
        name="reducer",
    )(tokens, grads, vw, gw, wgrad, stats)


def shards(tokens, value_act, gate_act, cotangent, value_weight, gate_weight,
           norm_gain, norm_bias, mix_weight, mix_bias):
    grads, wgrad, stats = mixer_call(
        value_act[0], gate_act[0], cotangent[0], norm_gain[None], norm_bias[None], mix_weight, mix_bias)
    tgrad, vout, gout, mixout, statout = reducer_call(
        tokens[0], grads, value_weight, gate_weight, wgrad, stats)
    return (tgrad[None], vout, gout, mixout, statout[0:16],
            statout[16:24].reshape(1024), statout[24:32].reshape(1024))


def solution(mesh):
    rows = P("dp", "sp", None)
    placed = (rows, rows, rows, rows, P("dp", None), P("dp", None), P(), P(), P(), P())
    return jax.shard_map(
        shards, mesh=mesh, in_specs=placed,
        out_specs=(rows, P("dp", None), P("dp", None), P(), P(), P(), P()), check_vma=False)
```

```python
import functools
import jax
import jax.numpy as jnp
from jax import lax
from jax.experimental import pallas as pl
from jax.experimental.pallas import tpu as pltpu
from jax.sharding import PartitionSpec as P

EPSILON = 1e-06
F32, BF16 = jnp.float32, jnp.bfloat16
NT = (((1,), (1,)), ((), ()))
TN = (((0,), (0,)), ((), ()))
NN = (((1,), (0,)), ((), ()))


TOP = 96
GATE_UNROLL = 4
LAST_UNROLL = 4
PROFILE = False
_open = []


def mark(name):
    if not PROFILE:
        return
    while _open:
        _open.pop().__exit__(None, None, None)
    if name:
        scope = jax.named_scope(name)
        scope.__enter__()
        _open.append(scope)


def dot(a, b, dims=NN):
    return lax.dot_general(a, b, dims, preferred_element_type=F32)


def split3(v):
    hi = v.astype(BF16)
    rest = v - hi.astype(F32)
    mid = rest.astype(BF16)
    low = (rest - mid.astype(F32)).astype(BF16)
    return hi, mid, low


def phi_terms(v):
    cdf = 0.5 * (1.0 + lax.erf(v * 0.7071067811865476))
    pdf = jnp.exp(-0.5 * v * v) * 0.3989422804014327
    return cdf, cdf + v * pdf


def fused(tokens, va_h, ga_h, cot_h, vw, gw, mixw_h, gain_h, bias_h, mixb_h,
          tgrad_h, wout_h, mixo_h, bout_h, nout_h, hout_h,
          tgrad, wout, mixo, bout, nout, hout, gain, bias, mixb,
          va, ga, cot, mixw, tokl, mcat, mtrn, normed, slope, spread, low, cv, gnorm, inv, gsum, bfull, acc_g, acc_b,
          grads, wgrad, stats,
          tokr, tt, wbuf,
          sfar, sup, sdn, fup, fdn, own1, agg, rlay, rprev, rnext, s1f, s1b, r2, own2, s2b, r3, fin, allf,
          mrecv, mq, mqb, mr1, mq1, mq1b, mr2, my, maz, max_, macc, mpart, mrp,
          stc, stx, sty, stz, stg, st0, st1,
          loc, outs, tok_s, tok_r, grd_s, grd_r, ring_s, ring_r, help_s, help_r, pair_s, pair_r, one_s, one_r, two_s, two_r,
          thr_s, thr_r, fou_s, fou_r, mix_s, mix_r, sts_s, sts_r):
    sp = lax.axis_index("sp")
    dp = lax.axis_index("dp")
    y, x = sp // 4, lax.rem(sp, 4)
    z, c = dp // 2, lax.rem(dp, 2)
    pc = 1 - c

    def at(nx=None, ny=None, nz=None, nc=None):
        nx = x if nx is None else nx
        ny = y if ny is None else ny
        nz = z if nz is None else nz
        nc = c if nc is None else nc
        return {"sp": ny * 4 + nx, "dp": nz * 2 + nc}

    def along(axis, k):
        if axis == "x":
            return at(nx=lax.rem(x + k, 4))
        if axis == "y":
            return at(ny=lax.rem(y + k, 4))
        return at(nz=lax.rem(z + k, 8))

    def copy(src, dst, ssem, rsem, to):
        return pltpu.make_async_remote_copy(
            src_ref=src, dst_ref=dst, send_sem=ssem, recv_sem=rsem,
            device_id=to, device_id_type=pl.DeviceIdType.MESH)

    def await_recv(dst, ssem, rsem):
        copy(dst, dst, ssem, rsem, at(nc=pc)).wait_recv()

    def await_send(src, ssem, rsem):
        copy(src, src, ssem, rsem, at(nc=pc)).wait_send()


    mark("barrier")
    barrier = pltpu.get_barrier_semaphore()
    pl.semaphore_signal(barrier, inc=1, device_id=at(nc=pc), device_id_type=pl.DeviceIdType.MESH)
    for k in range(1, 8):
        pl.semaphore_signal(barrier, inc=1, device_id=along("z", k), device_id_type=pl.DeviceIdType.MESH)
    for k in range(1, 16):
        pl.semaphore_signal(barrier, inc=1, device_id={"sp": lax.rem(sp + k, 16), "dp": dp},
                            device_id_type=pl.DeviceIdType.MESH)
    shard = (vw, gw)
    local = [pltpu.make_async_copy(va_h, va, loc.at[0]), pltpu.make_async_copy(cot_h, cot, loc.at[1]),
             pltpu.make_async_copy(ga_h, ga, loc.at[2])]
    for v in range(2):
        local.append(pltpu.make_async_copy(shard[v], wbuf.at[z, v, c], loc.at[3 + v]))
    for k in range(8):
        lanes = pl.ds(pl.multiple_of((2 * k + c) * 128, 128), 128)
        local.append(pltpu.make_async_copy(tokens.at[:, lanes], tokl.at[k], loc.at[5 + k]))
    local.append(pltpu.make_async_copy(mixw_h, mixw, loc.at[13]))
    local.append(pltpu.make_async_copy(gain_h, gain, loc.at[14]))
    local.append(pltpu.make_async_copy(bias_h, bias, loc.at[15]))
    local.append(pltpu.make_async_copy(mixb_h, mixb, loc.at[16]))
    for n in (0, 1, 2, 14, 15, 16, 13, 5, 6, 7, 8, 9, 10, 11, 12, 3, 4):
        local[n].start()

    axes = ("x", "y")
    place = (x, y)

    def top(zz, v, cc):
        return wbuf.at[zz, v, cc, pl.ds(0, TOP)]

    def low_rows(zz, v, cc):
        return wbuf.at[zz, v, cc, pl.ds(TOP, 128 - TOP)]

    def slice_of(zz, v, cc):
        return wbuf.at[zz, v, cc, pl.ds(TOP, 128 - TOP), pl.ds(pl.multiple_of(place[v] * 256, 256), 256)]

    def came_from(direction, h):
        return lax.rem(z - h + 8, 8) if direction == 0 else lax.rem(z + h, 8)

    def last_hop(direction, v):
        return 4 if direction == v else 3

    def number(direction, v, h):
        return (direction * 2 + v) * 4 + h - 1

    def hop(direction, v, h, part):
        origin = came_from(direction, h - 1)
        dst = (top, slice_of)[part](origin, v, c)
        if h > 1:
            src = dst
        elif part == 0:
            src = shard[v].at[pl.ds(0, TOP)]
        else:
            src = shard[v].at[pl.ds(TOP, 128 - TOP), pl.ds(pl.multiple_of(place[v] * 256, 256), 256)]
        i = number(direction, v, h) + 16 * part
        return copy(src, dst, ring_s.at[i], ring_r.at[i], along("z", 1 if direction == 0 else 7))

    def directions(h, v):
        return [d for d in range(2) if h <= last_hop(d, v)]

    def ring_part(h, v, part):
        for d in directions(h, v):
            hop(d, v, h, part).wait_recv()
            if h < last_hop(d, v):
                hop(d, v, h + 1, part).start()

    def ring_step(h, v):
        if h > 1:
            ring_part(h, v, 1)
        ring_part(h, v, 0)
        for d in directions(h, v):
            ref = top(came_from(d, h), v, c)
            i = 2 + number(d, v, h)
            copy(ref, ref, pair_s.at[i], pair_r.at[i], at(nc=pc)).start()

    def help_out(h, v):
        for d in directions(h, v):
            i = number(d, v, h)
            ref = slice_of(came_from(d, h), v, c)
            for k in range(1, 4):
                copy(ref, ref, help_s.at[i], help_r.at[i], along(axes[v], k)).start()

    def helped(d, v, h):
        ref = wbuf.at[0, v, 0, pl.ds(TOP, 128 - TOP), pl.ds(0, 768)]
        return copy(ref, ref, help_s.at[number(d, v, h)], help_r.at[number(d, v, h)], at(nc=pc))

    def help_pair(h):
        for v in range(2):
            for d in directions(h, v):
                helped(d, v, h).wait_recv()
                ref = low_rows(came_from(d, h), v, c)
                i = 18 + number(d, v, h)
                copy(ref, ref, pair_s.at[i], pair_r.at[i], at(nc=pc)).start()

    def await_pair(h):
        for v in range(2):
            if h == 0:
                await_recv(wbuf.at[0, v, 0], pair_s.at[v], pair_r.at[v])
                continue
            for d in directions(h, v):
                i = number(d, v, h)
                await_recv(top(0, v, 0), pair_s.at[2 + i], pair_r.at[2 + i])
                await_recv(low_rows(0, v, 0), pair_s.at[18 + i], pair_r.at[18 + i])

    def into_tokens(zz):
        wv = wbuf[zz, 0].reshape(256, 1024)
        wg = wbuf[zz, 1].reshape(256, 1024)
        out = dot(grads[0:384, 0:1024], wv, NT) + dot(grads[0:384, 1024:2048], wg, NT)
        tgrad[:, pl.ds(pl.multiple_of(zz * 256, 256), 256)] = out.astype(BF16)

    rows = 16
    row = lax.broadcasted_iota(jnp.int32, (128, 128), 0)
    col = lax.broadcasted_iota(jnp.int32, (128, 128), 1)
    keep = row >= col

    gsum[...] = jnp.zeros_like(gsum)
    acc_g[...] = jnp.zeros_like(acc_g)
    acc_b[...] = jnp.zeros_like(acc_b)
    mark("m_value")
    local[0].wait()
    local[1].wait()
    def first(i, _):
        at = pl.ds(pl.multiple_of(i * rows, rows), rows)
        v = va[at, :].astype(F32)
        cdf, slp = phi_terms(v)
        c = cot[at, :].astype(F32)
        gs = c * (v * cdf)
        low[at, :] = gs.astype(BF16)
        cv[at, :] = c * slp
        inb = pl.ds(pl.multiple_of(lax.rem(i, 8) * rows, rows), rows)
        gsum[inb, :] += gs
        return 0

    lax.fori_loop(0, 24, first, 0)

    mark("barrierwait")
    pl.semaphore_wait(barrier, 23)
    for part in (1, 0):
        for v in range(2):
            for direction in range(2):
                hop(direction, v, 1, part).start()
    for k in range(8):
        lanes = pl.ds(pl.multiple_of((2 * k + pc) * 128, 128), 128)
        copy(tokens.at[:, lanes], tokr.at[k], tok_s.at[0], tok_r.at[0], at(nc=pc)).start()
    for v in range(2):
        copy(shard[v], wbuf.at[z, v, c], pair_s.at[v], pair_r.at[v], at(nc=pc)).start()

    mark("m_gate")
    local[2].wait()
    local[14].wait()
    local[15].wait()
    def second(i, _):
        for u in range(GATE_UNROLL):
            rat = pl.ds(pl.multiple_of((i * GATE_UNROLL + u) * rows, rows), rows)
            v = ga[rat, :].astype(F32)
            cdf, slp = phi_terms(v)
            slope[rat, :] = slp
            g = v * cdf
            cen = g - jnp.mean(g, axis=-1, keepdims=True)
            s = lax.rsqrt(jnp.mean(cen * cen, axis=-1, keepdims=True) + EPSILON)
            n = cen * s
            normed[rat, :] = n
            inv[rat, :] = jnp.broadcast_to(s, (rows, 128))
            spread[rat, :] = (n * gain[...] + bias[...]).astype(BF16)
        return 0

    lax.fori_loop(0, 24 // GATE_UNROLL, second, 0)

    mark("m_prep")
    local[13].wait()
    def prep(p, _):
        for h in range(2):
            m = jnp.where(keep, mixw[2 * p + h].astype(F32), 0.0)
            mcat[p, :, h * 128:(h + 1) * 128] = m.astype(BF16)
            mtrn[p, :, h * 128:(h + 1) * 128] = m.T.astype(BF16)
        return 0

    lax.fori_loop(0, 8, prep, 0)
    group = lax.broadcasted_iota(jnp.int32, (16, 1024), 0)
    chan = lax.broadcasted_iota(jnp.int32, (16, 1024), 1) // 64
    pick = jnp.where(group == chan, 1.0, 0.0).astype(BF16)
    local[16].wait()
    parts = split3(mixb[...])
    bfull[...] = dot(parts[0], pick, TN) + dot(parts[1], pick, TN) + dot(parts[2], pick, TN)

    mark("transpose")
    for k in range(8):
        local[5 + k].wait()
        tt[k * 128:(k + 1) * 128, 0:384] = tokl[k].T
    await_recv(tokr, tok_s.at[0], tok_r.at[0])
    for k in range(8):
        tt[k * 128:(k + 1) * 128, 384:768] = tokr[k].T
    mark("help1")
    for v in range(2):
        ring_part(1, v, 1)
        help_out(1, v)
    mark("m_mix")
    lane = lax.broadcasted_iota(jnp.int32, (1, 128), 1)
    m0 = jnp.where(lane < 64, 1.0, 0.0).astype(BF16)
    m1 = jnp.where(lane < 64, 0.0, 1.0).astype(BF16)

    def mix(p, _):
        cols = pl.ds(pl.multiple_of(p * 128, 128), 128)
        wg = None
        for b in range(3):
            r = slice(b * 128, (b + 1) * 128)
            s = spread[r, cols]
            l = low[r, cols]
            stack_s = jnp.concatenate((s * m0, s * m1), axis=0)
            stack_l = jnp.concatenate((l * m0, l * m1), axis=0)
            spatial = dot(mcat[p], stack_s) + bfull[:, cols]
            grads[r, cols] = (cv[r, cols] * spatial).astype(BF16)
            gnorm[r, cols] = dot(mtrn[p], stack_l)
            term = dot(stack_l, s, NT)
            wg = term if wg is None else wg + term
        wgrad[2 * p] = jnp.where(keep, wg[:128], 0.0)
        wgrad[2 * p + 1] = jnp.where(keep, wg[128:], 0.0)
        return 0

    lax.fori_loop(0, 8, mix, 0)

    def swap(h):
        lanes = pl.ds(h * 1024, 1024)
        return copy(grads.at[pl.ds(0, 384), lanes], grads.at[pl.ds(384, 384), lanes], grd_s.at[h], grd_r.at[h], at(nc=pc))

    swap(0).start()
    for k in range(8):
        copy(wgrad.at[2 * k + pc], mrecv.at[k], mix_s.at[0], mix_r.at[0], at(nc=pc)).start()

    mark("m_last")
    def last(i, _):
        for u in range(LAST_UNROLL):
            rat = pl.ds(pl.multiple_of((i * LAST_UNROLL + u) * rows, rows), rows)
            gn = gnorm[rat, :]
            n = normed[rat, :]
            gnn = gn * n
            acc_g[...] += gnn
            acc_b[...] += gn
            h = gn * gain[...]
            mean_h = jnp.mean(h, axis=-1, keepdims=True)
            mean_hn = jnp.mean(h * n, axis=-1, keepdims=True)
            s = inv[rat, 0:1]
            out = s * (h - mean_h - n * mean_hn)
            grads[rat, 1024:2048] = (out * slope[rat, :]).astype(BF16)
        return 0

    lax.fori_loop(0, 24 // LAST_UNROLL, last, 0)
    swap(1).start()
    mark("m_stats")
    parts = split3(gsum[...])
    stats[0:16, :] = dot(pick, parts[0], NT) + dot(pick, parts[1], NT) + dot(pick, parts[2], NT)
    tot_g = jnp.sum(acc_g[...], axis=0, keepdims=True)
    tot_b = jnp.sum(acc_b[...], axis=0, keepdims=True)
    for k in range(8):
        stats[16 + k:17 + k, :] = tot_g[:, k * 128:(k + 1) * 128]
        stats[24 + k:25 + k, :] = tot_b[:, k * 128:(k + 1) * 128]
    copy(stats, stc, sts_s.at[0], sts_r.at[0], at(nc=pc)).start()
    def product(h, dest, half):
        wide = pl.ds(pl.multiple_of(h * 1024 + dest * 256, 256), 256)
        return dot(tt[half * 512:(half + 1) * 512, :], grads[:, wide]).reshape(2, 256, 256)

    def one(i, h, src, dst, k):
        return copy(src, dst, one_s.at[h * 6 + i], one_r.at[h * 6 + i], along(axes[h], k))

    def far_tiles(h):
        mark(f"far{h}")
        dest = lax.rem(place[h] + 2, 4)
        sfar[h, 0:2] = product(h, dest, 0).astype(BF16)
        one(0, h, sfar.at[h, 0:2], rlay.at[h, 0], 1).start()
        sfar[h, 2:4] = product(h, dest, 1).astype(BF16)
        one(1, h, sfar.at[h, 2:4], rlay.at[h, 1], 3).start()

    def near_tiles(h):
        mark(f"near{h}")
        up, dn = lax.rem(place[h] + 1, 4), lax.rem(place[h] + 3, 4)
        sup[h, 2:4] = product(h, up, 1).astype(BF16)
        one(2, h, sup.at[h, 2:4], rprev.at[h, 1], 1).start()
        sdn[h, 0:2] = product(h, dn, 0).astype(BF16)
        one(3, h, sdn.at[h, 0:2], rnext.at[h, 0], 3).start()
        fup[h, 0:2] = product(h, up, 0)
        fdn[h, 2:4] = product(h, dn, 1)

    def own_tiles(h):
        mark(f"own{h}")
        own1[h, 0:2] = product(h, place[h], 0)
        own1[h, 2:4] = product(h, place[h], 1)

    def relay(h):
        mark(f"relay{h}")
        one(0, h, rlay.at[h, 0], rlay.at[h, 0], 1).wait_recv()
        agg[h, 0] = (fup[h, 0:2] + rlay[h, 0].astype(F32)).astype(BF16)
        one(4, h, agg.at[h, 0], rprev.at[h, 0], 1).start()
        one(1, h, rlay.at[h, 1], rlay.at[h, 1], 3).wait_recv()
        agg[h, 1] = (fdn[h, 2:4] + rlay[h, 1].astype(F32)).astype(BF16)
        one(5, h, agg.at[h, 1], rnext.at[h, 1], 3).start()

    def stats_x():
        mark("stats_x")
        await_recv(stc, sts_s.at[0], sts_r.at[0])
        st0[...] = (stats[...] + stc[...]).reshape(4, 8, 128)
        for k in range(1, 4):
            copy(st0.at[lax.rem(x + k, 4)], stx.at[k - 1], sts_s.at[1], sts_r.at[1], along("x", k)).start()

    def stats_y():
        mark("stats_y")
        await_recv(stx, sts_s.at[1], sts_r.at[1])
        st1[0] = ((st0[x] + stx[0]) + stx[1]) + stx[2]
        sty[y] = st1[0]
        for k in range(1, 4):
            copy(st1.at[0], sty.at[y], sts_s.at[2], sts_r.at[2], along("y", k)).start()

    def stats_z():
        mark("stats_z")
        await_recv(sty.at[pl.ds(0, 3)], sts_s.at[2], sts_r.at[2])
        st1[1] = (sty[0] + sty[1]) + (sty[2] + sty[3])
        stz[z] = st1[1]
        for k in range(1, 8):
            copy(st1.at[1], stz.at[z], sts_s.at[3], sts_r.at[3], along("z", k)).start()

    def stats_back():
        mark("stats_back")
        await_recv(stz.at[pl.ds(0, 7)], sts_s.at[3], sts_r.at[3])
        t = stz[0]
        for k in range(1, 8):
            t = t + stz[k]
        st1[2] = t
        stg[x] = t
        for k in range(1, 4):
            copy(st1.at[2], stg.at[x], sts_s.at[4], sts_r.at[4], along("x", k)).start()

    def stats_end():
        mark("stats_end")
        await_recv(stg.at[pl.ds(0, 3)], sts_s.at[4], sts_r.at[4])
        bout[0:8] = stg[0]
        bout[8:16] = stg[1]
        nout[...] = stg[2]
        hout[...] = stg[3]
        for n in (3, 4, 5):
            put[n].start()

    def mix_z():
        mark("mix_z")
        await_recv(mrecv, mix_s.at[0], mix_r.at[0])
        for k in range(8):
            v = wgrad[2 * k + c] + mrecv[k]
            mq[k] = v
            mqb[k] = v.astype(BF16)
        for k in range(1, 8):
            copy(mqb.at[lax.rem(z + k, 8)], mr2.at[k - 1], mix_s.at[1], mix_r.at[1], along("z", k)).start()

    def mix_x():
        mark("mix_x")
        await_recv(mr2, mix_s.at[1], mix_r.at[1])
        v = mq[z]
        for k in range(7):
            v = v + mr2[k].astype(F32)
        v = v.reshape(4, 32, 128)
        mq1[...] = v
        mq1b[...] = v.astype(BF16)
        for k in range(1, 4):
            copy(mq1b.at[lax.rem(x + k, 4)], mr1.at[k - 1], mix_s.at[2], mix_r.at[2], along("x", k)).start()

    def mix_y():
        mark("mix_y")
        await_recv(mr1, mix_s.at[2], mix_r.at[2])
        v = mq1[x] + (mr1[0].astype(F32) + mr1[1].astype(F32)) + mr1[2].astype(F32)
        mpart[...] = v
        my[y] = v
        for k in range(1, 4):
            copy(mpart, my.at[y], mix_s.at[3], mix_r.at[3], along("y", k)).start()

    def mix_back_z():
        mark("mix_back_z")
        await_recv(my.at[pl.ds(0, 3)], mix_s.at[3], mix_r.at[3])
        v = ((my[0] + my[1]) + (my[2] + my[3])).astype(BF16)
        macc[...] = v
        maz[z] = v
        for k in range(1, 8):
            copy(macc, maz.at[z], mix_s.at[4], mix_r.at[4], along("z", k)).start()

    def mix_back_x():
        mark("mix_back_x")
        await_recv(maz.at[pl.ds(0, 7)], mix_s.at[4], mix_r.at[4])
        max_[x] = maz[...]
        for k in range(1, 4):
            copy(maz, max_.at[x], mix_s.at[5], mix_r.at[5], along("x", k)).start()

    def mix_back_c():
        mark("mix_back_c")
        await_recv(max_.at[pl.ds(0, 3)], mix_s.at[5], mix_r.at[5])
        copy(max_, mrp, mix_s.at[6], mix_r.at[6], at(nc=pc)).start()

    def mix_end():
        mark("mix_end")
        await_recv(mrp, mix_s.at[6], mix_r.at[6])
        for k in range(8):
            mixo[2 * k + c] = max_[:, k].reshape(128, 128)
            mixo[2 * k + pc] = mrp[:, k].reshape(128, 128)
        put[2].start()

    def ring(h, v):
        mark(f"ring{h}{v}")
        ring_step(h, v)

    def into(h):
        mark(f"into{h}")
        await_pair(h)
        if h == 0:
            local[3].wait()
            local[4].wait()
            into_tokens(z)
            return
        into_tokens(lax.rem(z + h, 8))
        if h < 4:
            into_tokens(lax.rem(z + 8 - h, 8))

    put = [pltpu.make_async_copy(tgrad, tgrad_h, outs.at[0]), pltpu.make_async_copy(wout.at[0], wout_h.at[0], outs.at[1]),
           pltpu.make_async_copy(mixo, mixo_h, outs.at[2]), pltpu.make_async_copy(bout, bout_h, outs.at[3]),
           pltpu.make_async_copy(nout, nout_h, outs.at[4]), pltpu.make_async_copy(hout, hout_h, outs.at[5]),
           pltpu.make_async_copy(wout.at[1], wout_h.at[1], outs.at[6])]

    def stage_two(h):
        mark(f"two{h}")
        for i, buf in ((2, rprev.at[h, 1]), (4, rprev.at[h, 0]), (3, rnext.at[h, 0]), (5, rnext.at[h, 1])):
            one(i, h, buf, buf, 1).wait_recv()
        for q in range(4):
            v = own1[h, q] + (rprev[h, q // 2, q % 2].astype(F32) + rnext[h, q // 2, q % 2].astype(F32))
            v = v.reshape(2, 4, 32, 256)
            s1f[h, 2 * q:2 * q + 2] = v
            s1b[h, 2 * q:2 * q + 2] = v.astype(BF16)
        other = place[1 - h]
        for k in range(1, 4):
            copy(s1b.at[h, :, lax.rem(other + k, 4)], r2.at[h, k - 1], two_s.at[h], two_r.at[h],
                 along(axes[1 - h], k)).start()

    def stage_three(h):
        mark(f"three{h}")
        await_recv(r2.at[h], two_s.at[h], two_r.at[h])
        v = s1f[h, :, place[1 - h]] + (r2[h, 0].astype(F32) + r2[h, 1].astype(F32)) + r2[h, 2].astype(F32)
        own2[h] = v
        s2b[h] = v.astype(BF16)
        for k in range(1, 8):
            copy(s2b.at[h, lax.rem(z + k, 8)], r3.at[h, k - 1], thr_s.at[h], thr_r.at[h], along("z", k)).start()

    def stage_four(h):
        mark(f"four{h}")
        await_recv(r3.at[h], thr_s.at[h], thr_r.at[h])
        v = own2[h, z]
        for k in range(7):
            v = v + r3[h, k].astype(F32)
        fin[h] = v.astype(BF16)
        allf[h, sp] = v.astype(BF16)
        for k in range(1, 16):
            copy(fin.at[h], allf.at[h, sp], fou_s.at[h], fou_r.at[h], {"sp": lax.rem(sp + k, 16), "dp": dp}).start()

    def stage_end(h):
        mark(f"end{h}")
        await_recv(allf.at[h, pl.ds(0, 15)], fou_s.at[h], fou_r.at[h])
        for s in range(16):
            a, b = (s // 4, s % 4) if h == 0 else (s % 4, s // 4)
            wout[h, a * 32:(a + 1) * 32, b * 256:(b + 1) * 256] = allf[h, s]
        put[(1, 6)[h]].start()

    swap(0).wait_recv()
    far_tiles(0)
    ring(1, 0)
    swap(1).wait_recv()
    far_tiles(1)
    mix_z()
    ring(1, 1)
    near_tiles(0)
    near_tiles(1)
    stats_x()
    own_tiles(0)
    own_tiles(1)
    relay(0)
    relay(1)
    ring(2, 0)
    into(0)
    ring(2, 1)
    help_pair(1)
    into(1)
    ring(3, 0)
    stage_two(0)
    stage_two(1)
    stats_y()
    mix_x()
    for v in range(2):
        help_out(2, v)
    ring(3, 1)
    stage_three(0)
    stage_three(1)
    mix_y()
    stats_z()
    for v in range(2):
        help_out(3, v)
    mark("help_pair2")
    help_pair(2)
    into(2)
    ring(4, 0)
    ring(4, 1)
    for v in range(2):
        help_out(4, v)
    mix_back_z()
    stage_four(0)
    stage_four(1)
    mark("help_pair3")
    help_pair(3)
    into(3)
    mix_back_x()
    stats_back()
    mark("help_pair4")
    help_pair(4)
    into(4)
    put[0].start()
    mix_back_c()
    stats_end()
    mix_end()
    stage_end(0)
    stage_end(1)

    mark("sends")
    for one_out in put:
        one_out.wait()
    await_send(tokr, tok_s.at[0], tok_r.at[0])
    for h in range(2):
        swap(h).wait_send()
        for i in range(6):
            await_send(agg.at[h, 0], one_s.at[h * 6 + i], one_r.at[h * 6 + i])
        await_send(r2.at[h], two_s.at[h], two_r.at[h])
        await_send(r3.at[h], thr_s.at[h], thr_r.at[h])
        await_send(allf.at[h, pl.ds(0, 15)], fou_s.at[h], fou_r.at[h])
    for i, buf in enumerate((mrecv, mr2, mr1, my.at[pl.ds(0, 3)], maz.at[pl.ds(0, 7)],
                             max_.at[pl.ds(0, 3)], mrp)):
        await_send(buf, mix_s.at[i], mix_r.at[i])
    for i, buf in enumerate((stc, stx, sty.at[pl.ds(0, 3)], stz.at[pl.ds(0, 7)], stg.at[pl.ds(0, 3)])):
        await_send(buf, sts_s.at[i], sts_r.at[i])
    for v in range(2):
        await_send(shard[v], pair_s.at[v], pair_r.at[v])
        for h in range(1, 5):
            for d in directions(h, v):
                i = number(d, v, h)
                hop(d, v, h, 0).wait_send()
                hop(d, v, h, 1).wait_send()
                helped(d, v, h).wait_send()
                await_send(top(0, v, 0), pair_s.at[2 + i], pair_r.at[2 + i])
                await_send(low_rows(0, v, 0), pair_s.at[18 + i], pair_r.at[18 + i])
    mark(None)


SCRATCH = (
    pltpu.VMEM((384, 2048), BF16),
    pltpu.VMEM((2, 128, 1024), BF16),
    pltpu.VMEM((16, 128, 128), BF16),
    pltpu.VMEM((16, 128), F32),
    pltpu.VMEM((8, 128), F32),
    pltpu.VMEM((8, 128), F32),
    pltpu.VMEM((1, 1024), F32),
    pltpu.VMEM((1, 1024), F32),
    pltpu.VMEM((16, 128), F32),
    pltpu.VMEM((384, 1024), BF16),
    pltpu.VMEM((384, 1024), BF16),
    pltpu.VMEM((384, 1024), BF16),
    pltpu.VMEM((16, 128, 128), BF16),
    pltpu.VMEM((8, 384, 128), BF16),
    pltpu.VMEM((8, 128, 256), BF16),
    pltpu.VMEM((8, 128, 256), BF16),
    pltpu.VMEM((384, 1024), F32),
    pltpu.VMEM((384, 1024), F32),
    pltpu.VMEM((384, 1024), BF16),
    pltpu.VMEM((384, 1024), BF16),
    pltpu.VMEM((384, 1024), F32),
    pltpu.VMEM((384, 1024), F32),
    pltpu.VMEM((384, 128), F32),
    pltpu.VMEM((128, 1024), F32),
    pltpu.VMEM((128, 1024), F32),
    pltpu.VMEM((16, 1024), F32),
    pltpu.VMEM((16, 1024), F32),
    pltpu.VMEM((768, 2048), BF16),
    pltpu.VMEM((16, 128, 128), F32),
    pltpu.VMEM((32, 128), F32),
    pltpu.VMEM((8, 384, 128), BF16),
    pltpu.VMEM((1024, 768), BF16),
    pltpu.VMEM((8, 2, 2, 128, 1024), BF16),
    pltpu.VMEM((2, 4, 256, 256), BF16),
    pltpu.VMEM((2, 4, 256, 256), BF16),
    pltpu.VMEM((2, 4, 256, 256), BF16),
    pltpu.VMEM((2, 4, 256, 256), F32),
    pltpu.VMEM((2, 4, 256, 256), F32),
    pltpu.VMEM((2, 4, 256, 256), F32),
    pltpu.VMEM((2, 2, 2, 256, 256), BF16),
    pltpu.VMEM((2, 2, 2, 256, 256), BF16),
    pltpu.VMEM((2, 2, 2, 256, 256), BF16),
    pltpu.VMEM((2, 2, 2, 256, 256), BF16),
    pltpu.VMEM((2, 8, 4, 32, 256), F32),
    pltpu.VMEM((2, 8, 4, 32, 256), BF16),
    pltpu.VMEM((2, 3, 8, 32, 256), BF16),
    pltpu.VMEM((2, 8, 32, 256), F32),
    pltpu.VMEM((2, 8, 32, 256), BF16),
    pltpu.VMEM((2, 7, 32, 256), BF16),
    pltpu.VMEM((2, 32, 256), BF16),
    pltpu.VMEM((2, 16, 32, 256), BF16),
    pltpu.VMEM((8, 128, 128), F32),
    pltpu.VMEM((8, 128, 128), F32),
    pltpu.VMEM((8, 128, 128), BF16),
    pltpu.VMEM((3, 32, 128), BF16),
    pltpu.VMEM((4, 32, 128), F32),
    pltpu.VMEM((4, 32, 128), BF16),
    pltpu.VMEM((7, 128, 128), BF16),
    pltpu.VMEM((4, 32, 128), F32),
    pltpu.VMEM((8, 32, 128), BF16),
    pltpu.VMEM((4, 8, 32, 128), BF16),
    pltpu.VMEM((32, 128), BF16),
    pltpu.VMEM((32, 128), F32),
    pltpu.VMEM((4, 8, 32, 128), BF16),
    pltpu.VMEM((32, 128), F32),
    pltpu.VMEM((3, 8, 128), F32),
    pltpu.VMEM((4, 8, 128), F32),
    pltpu.VMEM((8, 8, 128), F32),
    pltpu.VMEM((4, 8, 128), F32),
    pltpu.VMEM((4, 8, 128), F32),
    pltpu.VMEM((3, 8, 128), F32),
    pltpu.SemaphoreType.DMA((17,)), pltpu.SemaphoreType.DMA((7,)),
    pltpu.SemaphoreType.DMA((1,)), pltpu.SemaphoreType.DMA((1,)),
    pltpu.SemaphoreType.DMA((2,)), pltpu.SemaphoreType.DMA((2,)),
    pltpu.SemaphoreType.DMA((32,)), pltpu.SemaphoreType.DMA((32,)),
    pltpu.SemaphoreType.DMA((16,)), pltpu.SemaphoreType.DMA((16,)),
    pltpu.SemaphoreType.DMA((34,)), pltpu.SemaphoreType.DMA((34,)),
    pltpu.SemaphoreType.DMA((12,)), pltpu.SemaphoreType.DMA((12,)),
    pltpu.SemaphoreType.DMA((2,)), pltpu.SemaphoreType.DMA((2,)),
    pltpu.SemaphoreType.DMA((2,)), pltpu.SemaphoreType.DMA((2,)),
    pltpu.SemaphoreType.DMA((2,)), pltpu.SemaphoreType.DMA((2,)),
    pltpu.SemaphoreType.DMA((7,)), pltpu.SemaphoreType.DMA((7,)),
    pltpu.SemaphoreType.DMA((5,)), pltpu.SemaphoreType.DMA((5,)),
)


def fused_call(tokens, va, ga, cot, vw, gw, mixw, gain, bias, mixb):
    hbm = pl.BlockSpec(memory_space=pl.ANY)
    return pl.pallas_call(
        fused,
        out_shape=(
            jax.ShapeDtypeStruct((384, 2048), BF16),
            jax.ShapeDtypeStruct((2, 128, 1024), BF16),
            jax.ShapeDtypeStruct((16, 128, 128), BF16),
            jax.ShapeDtypeStruct((16, 128), F32),
            jax.ShapeDtypeStruct((8, 128), F32),
            jax.ShapeDtypeStruct((8, 128), F32),
        ),
        in_specs=[hbm] * 10,
        out_specs=(hbm,) * 6,
        scratch_shapes=list(SCRATCH),
        compiler_params=pltpu.CompilerParams(
            collective_id=0, has_side_effects=True, vmem_limit_bytes=62 * 1024 * 1024),
        name="fused",
    )(tokens, va, ga, cot, vw, gw, mixw, gain, bias, mixb)


def finish(tgrad, wsum, mixs, bsum, nsum, hsum, tout, vout, gout, mout, bout, nout, hout,
           tbuf, wbuf, wide, mbuf, mwide, bbuf, nbuf, hbuf, isem, osem):
    small = ((bsum, bbuf, bout), (nsum, nbuf, nout), (hsum, hbuf, hout))
    gets = [pltpu.make_async_copy(wsum.at[0], wbuf.at[0], isem.at[0]), pltpu.make_async_copy(wsum.at[1], wbuf.at[1], isem.at[1]),
            pltpu.make_async_copy(mixs, mbuf, isem.at[2])]
    puts = [pltpu.make_async_copy(wide.at[0], vout, osem.at[0]), pltpu.make_async_copy(wide.at[1], gout, osem.at[1]),
            pltpu.make_async_copy(mwide, mout, osem.at[2])]
    for k, (src, buf, dst) in enumerate(small):
        gets.append(pltpu.make_async_copy(src, buf, isem.at[3 + k]))
        puts.append(pltpu.make_async_copy(buf, dst, osem.at[3 + k]))
    for k in range(4):
        rows = pl.ds(k * 96, 96)
        gets.append(pltpu.make_async_copy(tgrad.at[rows], tbuf.at[rows], isem.at[6 + k]))
        puts.append(pltpu.make_async_copy(tbuf.at[rows], tout.at[rows], osem.at[6 + k]))
    for get in gets:
        get.start()
    for k in range(2):
        gets[k].wait()
        wide[k] = wbuf[k].astype(F32)
        puts[k].start()
    gets[2].wait()
    mwide[...] = mbuf[...].astype(F32)
    puts[2].start()
    for k in range(3, 10):
        gets[k].wait()
        puts[k].start()
    for put in puts:
        put.wait()


def finish_call(*parts):
    hbm = pl.BlockSpec(memory_space=pl.ANY)
    return pl.pallas_call(
        finish,
        out_shape=(
            jax.ShapeDtypeStruct((384, 2048), BF16),
            jax.ShapeDtypeStruct((128, 1024), F32),
            jax.ShapeDtypeStruct((128, 1024), F32),
            jax.ShapeDtypeStruct((16, 128, 128), F32),
            jax.ShapeDtypeStruct((16, 128), F32),
            jax.ShapeDtypeStruct((8, 128), F32),
            jax.ShapeDtypeStruct((8, 128), F32),
        ),
        in_specs=[hbm] * 6,
        out_specs=(hbm,) * 7,
        scratch_shapes=[
            pltpu.VMEM((384, 2048), BF16),
            pltpu.VMEM((2, 128, 1024), BF16),
            pltpu.VMEM((2, 128, 1024), F32),
            pltpu.VMEM((16, 128, 128), BF16),
            pltpu.VMEM((16, 128, 128), F32),
            pltpu.VMEM((16, 128), F32),
            pltpu.VMEM((8, 128), F32),
            pltpu.VMEM((8, 128), F32),
            pltpu.SemaphoreType.DMA((10,)),
            pltpu.SemaphoreType.DMA((10,)),
        ],
        name="finish",
    )(*parts)


def shards(tokens, value_act, gate_act, cotangent, value_weight, gate_weight,
           norm_gain, norm_bias, mix_weight, mix_bias):
    parts = fused_call(
        tokens[0], value_act[0], gate_act[0], cotangent[0], value_weight, gate_weight,
        mix_weight, norm_gain[None], norm_bias[None], mix_bias)
    tgrad, vout, gout, mout, bout, nout, hout = finish_call(*parts)
    return tgrad[None], vout, gout, mout, bout, nout.reshape(1024), hout.reshape(1024)


def solution(mesh):
    rows = P("dp", "sp", None)
    placed = (rows, rows, rows, rows, P("dp", None), P("dp", None), P(), P(), P(), P())
    return jax.shard_map(
        shards, mesh=mesh, in_specs=placed,
        out_specs=(rows, P("dp", None), P("dp", None), P(), P(), P(), P()), check_vma=False)
```

```python
import functools
import jax
import jax.numpy as jnp
from jax import lax
from jax.experimental import pallas as pl
from jax.experimental.pallas import tpu as pltpu
from jax.sharding import PartitionSpec as P

EPSILON = 1e-06
F32, BF16 = jnp.float32, jnp.bfloat16
NT = (((1,), (1,)), ((), ()))
TN = (((0,), (0,)), ((), ()))
NN = (((1,), (0,)), ((), ()))


TOP = 96
GATE_UNROLL = 4
LAST_UNROLL = 4
PROFILE = False
_open = []


def mark(name):
    if not PROFILE:
        return
    while _open:
        _open.pop().__exit__(None, None, None)
    if name:
        scope = jax.named_scope(name)
        scope.__enter__()
        _open.append(scope)


def dot(a, b, dims=NN):
    return lax.dot_general(a, b, dims, preferred_element_type=F32)


def split3(v):
    hi = v.astype(BF16)
    rest = v - hi.astype(F32)
    mid = rest.astype(BF16)
    low = (rest - mid.astype(F32)).astype(BF16)
    return hi, mid, low


def phi_terms(v):
    cdf = 0.5 * (1.0 + lax.erf(v * 0.7071067811865476))
    pdf = jnp.exp(-0.5 * v * v) * 0.3989422804014327
    return cdf, cdf + v * pdf


def fused(tokens, va_h, ga_h, cot_h, vw, gw, mixw_h, gain_h, bias_h, mixb_h,
          tgrad, wout, mixo, bout, nout, hout, gain, bias, mixb,
          va, ga, cot, mixw, tokl, mcat, mtrn, normed, slope, spread, low, cv, gnorm, inv, gsum, bfull, acc_g, acc_b,
          grads, wgrad, stats,
          tokr, tt, wbuf,
          sfar, sup, sdn, fup, fdn, own1, agg, rlay, rprev, rnext, s1f, s1b, r2, own2, s2b, r3, fin, allf,
          mrecv, mq, mqb, mr1, mq1, mq1b, mr2, my, maz, max_, macc, mpart, mrp,
          stc, stx, sty, stz, stg, st0, st1,
          loc, tok_s, tok_r, grd_s, grd_r, ring_s, ring_r, help_s, help_r, pair_s, pair_r, one_s, one_r, two_s, two_r,
          thr_s, thr_r, fou_s, fou_r, mix_s, mix_r, sts_s, sts_r):
    sp = lax.axis_index("sp")
    dp = lax.axis_index("dp")
    y, x = sp // 4, lax.rem(sp, 4)
    z, c = dp // 2, lax.rem(dp, 2)
    pc = 1 - c

    def at(nx=None, ny=None, nz=None, nc=None):
        nx = x if nx is None else nx
        ny = y if ny is None else ny
        nz = z if nz is None else nz
        nc = c if nc is None else nc
        return {"sp": ny * 4 + nx, "dp": nz * 2 + nc}

    def along(axis, k):
        if axis == "x":
            return at(nx=lax.rem(x + k, 4))
        if axis == "y":
            return at(ny=lax.rem(y + k, 4))
        return at(nz=lax.rem(z + k, 8))

    def copy(src, dst, ssem, rsem, to):
        return pltpu.make_async_remote_copy(
            src_ref=src, dst_ref=dst, send_sem=ssem, recv_sem=rsem,
            device_id=to, device_id_type=pl.DeviceIdType.MESH)

    def await_recv(dst, ssem, rsem):
        copy(dst, dst, ssem, rsem, at(nc=pc)).wait_recv()

    def await_send(src, ssem, rsem):
        copy(src, src, ssem, rsem, at(nc=pc)).wait_send()


    mark("barrier")
    barrier = pltpu.get_barrier_semaphore()
    pl.semaphore_signal(barrier, inc=1, device_id=at(nc=pc), device_id_type=pl.DeviceIdType.MESH)
    for k in range(1, 8):
        pl.semaphore_signal(barrier, inc=1, device_id=along("z", k), device_id_type=pl.DeviceIdType.MESH)
    for k in range(1, 16):
        pl.semaphore_signal(barrier, inc=1, device_id={"sp": lax.rem(sp + k, 16), "dp": dp},
                            device_id_type=pl.DeviceIdType.MESH)
    shard = (vw, gw)
    local = [pltpu.make_async_copy(va_h, va, loc.at[0]), pltpu.make_async_copy(cot_h, cot, loc.at[1]),
             pltpu.make_async_copy(ga_h, ga, loc.at[2])]
    for v in range(2):
        local.append(pltpu.make_async_copy(shard[v], wbuf.at[z, v, c], loc.at[3 + v]))
    for k in range(8):
        lanes = pl.ds(pl.multiple_of((2 * k + c) * 128, 128), 128)
        local.append(pltpu.make_async_copy(tokens.at[:, lanes], tokl.at[k], loc.at[5 + k]))
    local.append(pltpu.make_async_copy(mixw_h, mixw, loc.at[13]))
    local.append(pltpu.make_async_copy(gain_h, gain, loc.at[14]))
    local.append(pltpu.make_async_copy(bias_h, bias, loc.at[15]))
    local.append(pltpu.make_async_copy(mixb_h, mixb, loc.at[16]))
    for n in (13, 16, 0, 1, 2, 14, 15, 5, 6, 7, 8, 9, 10, 11, 12, 3, 4):
        local[n].start()

    axes = ("x", "y")
    place = (x, y)

    def top(zz, v, cc):
        return wbuf.at[zz, v, cc, pl.ds(0, TOP)]

    def low_rows(zz, v, cc):
        return wbuf.at[zz, v, cc, pl.ds(TOP, 128 - TOP)]

    def slice_of(zz, v, cc):
        return wbuf.at[zz, v, cc, pl.ds(TOP, 128 - TOP), pl.ds(pl.multiple_of(place[v] * 256, 256), 256)]

    def came_from(direction, h):
        return lax.rem(z - h + 8, 8) if direction == 0 else lax.rem(z + h, 8)

    def last_hop(direction, v):
        return 4 if direction == v else 3

    def number(direction, v, h):
        return (direction * 2 + v) * 4 + h - 1

    def hop(direction, v, h, part):
        origin = came_from(direction, h - 1)
        dst = (top, slice_of)[part](origin, v, c)
        if h > 1:
            src = dst
        elif part == 0:
            src = shard[v].at[pl.ds(0, TOP)]
        else:
            src = shard[v].at[pl.ds(TOP, 128 - TOP), pl.ds(pl.multiple_of(place[v] * 256, 256), 256)]
        i = number(direction, v, h) + 16 * part
        return copy(src, dst, ring_s.at[i], ring_r.at[i], along("z", 1 if direction == 0 else 7))

    def directions(h, v):
        return [d for d in range(2) if h <= last_hop(d, v)]

    def ring_part(h, v, part):
        for d in directions(h, v):
            hop(d, v, h, part).wait_recv()
            if h < last_hop(d, v):
                hop(d, v, h + 1, part).start()

    def ring_step(h, v):
        if h > 1:
            ring_part(h, v, 1)
        ring_part(h, v, 0)
        for d in directions(h, v):
            ref = top(came_from(d, h), v, c)
            i = 2 + number(d, v, h)
            copy(ref, ref, pair_s.at[i], pair_r.at[i], at(nc=pc)).start()

    def help_out(h, v):
        for d in directions(h, v):
            i = number(d, v, h)
            ref = slice_of(came_from(d, h), v, c)
            for k in range(1, 4):
                copy(ref, ref, help_s.at[i], help_r.at[i], along(axes[v], k)).start()

    def helped(d, v, h):
        ref = wbuf.at[0, v, 0, pl.ds(TOP, 128 - TOP), pl.ds(0, 768)]
        return copy(ref, ref, help_s.at[number(d, v, h)], help_r.at[number(d, v, h)], at(nc=pc))

    def help_pair(h):
        for v in range(2):
            for d in directions(h, v):
                helped(d, v, h).wait_recv()
                ref = low_rows(came_from(d, h), v, c)
                i = 18 + number(d, v, h)
                copy(ref, ref, pair_s.at[i], pair_r.at[i], at(nc=pc)).start()

    def await_pair(h):
        for v in range(2):
            if h == 0:
                await_recv(wbuf.at[0, v, 0], pair_s.at[v], pair_r.at[v])
                continue
            for d in directions(h, v):
                i = number(d, v, h)
                await_recv(top(0, v, 0), pair_s.at[2 + i], pair_r.at[2 + i])
                await_recv(low_rows(0, v, 0), pair_s.at[18 + i], pair_r.at[18 + i])

    def into_tokens(zz):
        wv = wbuf[zz, 0].reshape(256, 1024)
        wg = wbuf[zz, 1].reshape(256, 1024)
        out = dot(grads[0:384, 0:1024], wv, NT) + dot(grads[0:384, 1024:2048], wg, NT)
        tgrad[:, pl.ds(pl.multiple_of(zz * 256, 256), 256)] = out.astype(BF16)

    rows = 16
    row = lax.broadcasted_iota(jnp.int32, (128, 128), 0)
    col = lax.broadcasted_iota(jnp.int32, (128, 128), 1)
    keep = row >= col

    gsum[...] = jnp.zeros_like(gsum)
    acc_g[...] = jnp.zeros_like(acc_g)
    acc_b[...] = jnp.zeros_like(acc_b)
    mark("m_prep")
    local[13].wait()
    def prep(p, _):
        for h in range(2):
            m = jnp.where(keep, mixw[2 * p + h].astype(F32), 0.0)
            mcat[p, :, h * 128:(h + 1) * 128] = m.astype(BF16)
            mtrn[p, :, h * 128:(h + 1) * 128] = m.T.astype(BF16)
        return 0

    lax.fori_loop(0, 8, prep, 0)
    group = lax.broadcasted_iota(jnp.int32, (16, 1024), 0)
    chan = lax.broadcasted_iota(jnp.int32, (16, 1024), 1) // 64
    pick = jnp.where(group == chan, 1.0, 0.0).astype(BF16)
    local[16].wait()
    parts = split3(mixb[...])
    bfull[...] = dot(parts[0], pick, TN) + dot(parts[1], pick, TN) + dot(parts[2], pick, TN)

    mark("barrierwait")
    pl.semaphore_wait(barrier, 23)
    for part in (1, 0):
        for v in range(2):
            for direction in range(2):
                hop(direction, v, 1, part).start()
    for k in range(8):
        lanes = pl.ds(pl.multiple_of((2 * k + pc) * 128, 128), 128)
        copy(tokens.at[:, lanes], tokr.at[k], tok_s.at[0], tok_r.at[0], at(nc=pc)).start()
    for v in range(2):
        copy(shard[v], wbuf.at[z, v, c], pair_s.at[v], pair_r.at[v], at(nc=pc)).start()

    mark("m_value")
    local[0].wait()
    local[1].wait()
    def first(i, _):
        at = pl.ds(pl.multiple_of(i * rows, rows), rows)
        v = va[at, :].astype(F32)
        cdf, slp = phi_terms(v)
        c = cot[at, :].astype(F32)
        gs = c * (v * cdf)
        low[at, :] = gs.astype(BF16)
        cv[at, :] = c * slp
        inb = pl.ds(pl.multiple_of(lax.rem(i, 8) * rows, rows), rows)
        gsum[inb, :] += gs
        return 0

    lax.fori_loop(0, 24, first, 0)

    mark("m_gate")
    local[2].wait()
    local[14].wait()
    local[15].wait()
    def second(i, _):
        for u in range(GATE_UNROLL):
            rat = pl.ds(pl.multiple_of((i * GATE_UNROLL + u) * rows, rows), rows)
            v = ga[rat, :].astype(F32)
            cdf, slp = phi_terms(v)
            slope[rat, :] = slp
            g = v * cdf
            cen = g - jnp.mean(g, axis=-1, keepdims=True)
            s = lax.rsqrt(jnp.mean(cen * cen, axis=-1, keepdims=True) + EPSILON)
            n = cen * s
            normed[rat, :] = n
            inv[rat, :] = jnp.broadcast_to(s, (rows, 128))
            spread[rat, :] = (n * gain[...] + bias[...]).astype(BF16)
        return 0

    lax.fori_loop(0, 24 // GATE_UNROLL, second, 0)

    mark("transpose")
    for k in range(8):
        local[5 + k].wait()
        tt[k * 128:(k + 1) * 128, 0:384] = tokl[k].T
    await_recv(tokr, tok_s.at[0], tok_r.at[0])
    for k in range(8):
        tt[k * 128:(k + 1) * 128, 384:768] = tokr[k].T
    mark("help1")
    for v in range(2):
        ring_part(1, v, 1)
        help_out(1, v)
    mark("m_mix")
    lane = lax.broadcasted_iota(jnp.int32, (1, 128), 1)
    m0 = jnp.where(lane < 64, 1.0, 0.0).astype(BF16)
    m1 = jnp.where(lane < 64, 0.0, 1.0).astype(BF16)

    def mix_pair(p):
        cols = pl.ds(pl.multiple_of(p * 128, 128), 128)
        wg = None
        for b in range(3):
            r = slice(b * 128, (b + 1) * 128)
            s = spread[r, cols]
            l = low[r, cols]
            stack_s = jnp.concatenate((s * m0, s * m1), axis=0)
            stack_l = jnp.concatenate((l * m0, l * m1), axis=0)
            spatial = dot(mcat[p], stack_s) + bfull[:, cols]
            grads[r, cols] = (cv[r, cols] * spatial).astype(BF16)
            gnorm[r, cols] = dot(mtrn[p], stack_l)
            term = dot(stack_l, s, NT)
            wg = term if wg is None else wg + term
        wgrad[2 * p] = jnp.where(keep, wg[:128], 0.0)
        wgrad[2 * p + 1] = jnp.where(keep, wg[128:], 0.0)

    reach = (2, 1, 3, 0)

    def swap(h, j):
        dest = lax.rem(place[h] + reach[j], 4)
        lanes = pl.ds(pl.multiple_of(h * 1024 + dest * 256, 256), 256)
        return copy(grads.at[pl.ds(0, 384), lanes], grads.at[pl.ds(384, 384), lanes],
                    grd_s.at[h * 4 + j], grd_r.at[h * 4 + j], at(nc=pc))

    def mix(j, _):
        dest = lax.rem(x + 2 + j, 4)
        mix_pair(2 * dest)
        mix_pair(2 * dest + 1)
        return 0

    mix(0, 0)
    swap(0, 0).start()
    lax.fori_loop(1, 4, mix, 0)
    for j in (1, 2, 3):
        swap(0, j).start()
    for k in range(8):
        copy(wgrad.at[2 * k + pc], mrecv.at[k], mix_s.at[0], mix_r.at[0], at(nc=pc)).start()

    mark("m_last")
    def last(i, _):
        for u in range(LAST_UNROLL):
            rat = pl.ds(pl.multiple_of((i * LAST_UNROLL + u) * rows, rows), rows)
            gn = gnorm[rat, :]
            n = normed[rat, :]
            gnn = gn * n
            acc_g[...] += gnn
            acc_b[...] += gn
            h = gn * gain[...]
            mean_h = jnp.mean(h, axis=-1, keepdims=True)
            mean_hn = jnp.mean(h * n, axis=-1, keepdims=True)
            s = inv[rat, 0:1]
            out = s * (h - mean_h - n * mean_hn)
            grads[rat, 1024:2048] = (out * slope[rat, :]).astype(BF16)
        return 0

    lax.fori_loop(0, 24 // LAST_UNROLL, last, 0)
    for j in range(4):
        swap(1, j).start()
    def stats_pair():
        mark("m_stats")
        parts = split3(gsum[...])
        stats[0:16, :] = dot(pick, parts[0], NT) + dot(pick, parts[1], NT) + dot(pick, parts[2], NT)
        tot_g = jnp.sum(acc_g[...], axis=0, keepdims=True)
        tot_b = jnp.sum(acc_b[...], axis=0, keepdims=True)
        for k in range(8):
            stats[16 + k:17 + k, :] = tot_g[:, k * 128:(k + 1) * 128]
            stats[24 + k:25 + k, :] = tot_b[:, k * 128:(k + 1) * 128]
        copy(stats, stc, sts_s.at[0], sts_r.at[0], at(nc=pc)).start()

    def product(h, j, half):
        swap_in(h, j)
        dest = lax.rem(place[h] + reach[j], 4)
        wide = pl.ds(pl.multiple_of(h * 1024 + dest * 256, 256), 256)
        v = dot(tt[half * 512:(half + 1) * 512, :], grads[:, wide])
        return v[:, :128], v[:, 128:]

    arrived = set()

    def swap_in(h, j):
        if (h, j) not in arrived:
            arrived.add((h, j))
            swap(h, j).wait_recv()

    def one(i, g, src, dst, k):
        return copy(src, dst, one_s.at[g * 6 + i], one_r.at[g * 6 + i], along(axes[g // 2], k))

    def far_tiles(h):
        mark(f"far{h}")
        for half, k in ((0, 1), (1, 3)):
            v = product(h, 0, half)
            for n in range(2):
                g = 2 * h + n
                sfar[g, half] = v[n].astype(BF16)
                one(half, g, sfar.at[g, half], rlay.at[g, half], k).start()

    def near_tiles(h):
        mark(f"near{h}")
        v = product(h, 1, 1)
        for n in range(2):
            g = 2 * h + n
            sup[g] = v[n].astype(BF16)
            one(2, g, sup.at[g], rprev.at[g, 1], 1).start()
        v = product(h, 2, 0)
        for n in range(2):
            g = 2 * h + n
            sdn[g] = v[n].astype(BF16)
            one(3, g, sdn.at[g], rnext.at[g, 0], 3).start()
        fup[2 * h], fup[2 * h + 1] = product(h, 1, 0)
        fdn[2 * h], fdn[2 * h + 1] = product(h, 2, 1)

    def own_tiles(h):
        mark(f"own{h}")
        for half in range(2):
            own1[2 * h, half], own1[2 * h + 1, half] = product(h, 3, half)

    def relay(g):
        mark(f"relay{g}")
        one(0, g, rlay.at[g, 0], rlay.at[g, 0], 1).wait_recv()
        agg[g, 0] = (fup[g] + rlay[g, 0].astype(F32)).astype(BF16)
        one(4, g, agg.at[g, 0], rprev.at[g, 0], 1).start()
        one(1, g, rlay.at[g, 1], rlay.at[g, 1], 3).wait_recv()
        agg[g, 1] = (fdn[g] + rlay[g, 1].astype(F32)).astype(BF16)
        one(5, g, agg.at[g, 1], rnext.at[g, 1], 3).start()

    def stats_x():
        mark("stats_x")
        await_recv(stc, sts_s.at[0], sts_r.at[0])
        st0[...] = (stats[...] + stc[...]).reshape(4, 8, 128)
        for k in range(1, 4):
            copy(st0.at[lax.rem(x + k, 4)], stx.at[k - 1], sts_s.at[1], sts_r.at[1], along("x", k)).start()

    def stats_y():
        mark("stats_y")
        await_recv(stx, sts_s.at[1], sts_r.at[1])
        st1[0] = ((st0[x] + stx[0]) + stx[1]) + stx[2]
        sty[y] = st1[0]
        for k in range(1, 4):
            copy(st1.at[0], sty.at[y], sts_s.at[2], sts_r.at[2], along("y", k)).start()

    def stats_z():
        mark("stats_z")
        await_recv(sty.at[pl.ds(0, 3)], sts_s.at[2], sts_r.at[2])
        st1[1] = (sty[0] + sty[1]) + (sty[2] + sty[3])
        stz[z] = st1[1]
        for k in range(1, 8):
            copy(st1.at[1], stz.at[z], sts_s.at[3], sts_r.at[3], along("z", k)).start()

    def stats_back():
        mark("stats_back")
        await_recv(stz.at[pl.ds(0, 7)], sts_s.at[3], sts_r.at[3])
        t = stz[0]
        for k in range(1, 8):
            t = t + stz[k]
        st1[2] = t
        stg[x] = t
        for k in range(1, 4):
            copy(st1.at[2], stg.at[x], sts_s.at[4], sts_r.at[4], along("x", k)).start()

    def stats_end():
        mark("stats_end")
        await_recv(stg.at[pl.ds(0, 3)], sts_s.at[4], sts_r.at[4])
        bout[0:8] = stg[0]
        bout[8:16] = stg[1]
        nout[...] = stg[2]
        hout[...] = stg[3]

    def mix_x():
        mark("mix_x")
        await_recv(mrecv, mix_s.at[0], mix_r.at[0])
        for k in range(8):
            v = (wgrad[2 * k + c] + mrecv[k]).reshape(4, 32, 128)
            mq[k] = v
            mqb[k] = v.astype(BF16)
        for k in range(1, 4):
            copy(mqb.at[:, lax.rem(x + k, 4)], mr1.at[k - 1], mix_s.at[1], mix_r.at[1], along("x", k)).start()

    def mix_z():
        mark("mix_z")
        await_recv(mr1, mix_s.at[1], mix_r.at[1])
        v = mq[:, x] + (mr1[0].astype(F32) + mr1[1].astype(F32)) + mr1[2].astype(F32)
        mq1[...] = v
        mq1b[...] = v.astype(BF16)
        for k in range(1, 8):
            copy(mq1b.at[lax.rem(z + k, 8)], mr2.at[k - 1], mix_s.at[2], mix_r.at[2], along("z", k)).start()

    def mix_y():
        mark("mix_y")
        await_recv(mr2, mix_s.at[2], mix_r.at[2])
        v = mq1[z]
        for k in range(7):
            v = v + mr2[k].astype(F32)
        mpart[...] = v
        my[y] = v
        for k in range(1, 4):
            copy(mpart, my.at[y], mix_s.at[3], mix_r.at[3], along("y", k)).start()

    def mix_back_z():
        mark("mix_back_z")
        await_recv(my.at[pl.ds(0, 3)], mix_s.at[3], mix_r.at[3])
        v = ((my[0] + my[1]) + (my[2] + my[3])).astype(BF16)
        macc[...] = v
        maz[z] = v
        for k in range(1, 8):
            copy(macc, maz.at[z], mix_s.at[4], mix_r.at[4], along("z", k)).start()

    def mix_back_x():
        mark("mix_back_x")
        await_recv(maz.at[pl.ds(0, 7)], mix_s.at[4], mix_r.at[4])
        max_[x] = maz[...]
        for k in range(1, 4):
            copy(maz, max_.at[x], mix_s.at[5], mix_r.at[5], along("x", k)).start()

    def mix_back_c():
        mark("mix_back_c")
        await_recv(max_.at[pl.ds(0, 3)], mix_s.at[5], mix_r.at[5])
        copy(max_, mrp, mix_s.at[6], mix_r.at[6], at(nc=pc)).start()

    def mix_end():
        mark("mix_end")
        await_recv(mrp, mix_s.at[6], mix_r.at[6])
        for k in range(8):
            mixo[2 * k + c] = max_[:, k].reshape(128, 128)
            mixo[2 * k + pc] = mrp[:, k].reshape(128, 128)

    def ring(h, v):
        mark(f"ring{h}{v}")
        ring_step(h, v)

    def into(h):
        mark(f"into{h}")
        await_pair(h)
        if h == 0:
            local[3].wait()
            local[4].wait()
            into_tokens(z)
            return
        into_tokens(lax.rem(z + h, 8))
        if h < 4:
            into_tokens(lax.rem(z + 8 - h, 8))

    def stage_two(g):
        mark(f"two{g}")
        for i, buf in ((2, rprev.at[g, 1]), (3, rnext.at[g, 0]), (4, rprev.at[g, 0]), (5, rnext.at[g, 1])):
            one(i, g, buf, buf, 1).wait_recv()
        for q in range(2):
            v = own1[g, q] + (rprev[g, q].astype(F32) + rnext[g, q].astype(F32))
            v = v.reshape(4, 4, 32, 128)
            s1f[g, 4 * q:4 * q + 4] = v
            s1b[g, 4 * q:4 * q + 4] = v.astype(BF16)
        h = g // 2
        other = place[1 - h]
        for k in (2, 1, 3):
            copy(s1b.at[g, :, lax.rem(other + k, 4)], r2.at[g, k - 1], two_s.at[g], two_r.at[g],
                 along(axes[1 - h], k)).start()

    def stage_three(g):
        mark(f"three{g}")
        await_recv(r2.at[g], two_s.at[g], two_r.at[g])
        v = s1f[g, :, place[1 - g // 2]] + (r2[g, 0].astype(F32) + r2[g, 1].astype(F32)) + r2[g, 2].astype(F32)
        own2[g] = v
        s2b[g] = v.astype(BF16)
        for k in (4, 3, 5, 2, 6, 1, 7):
            copy(s2b.at[g, lax.rem(z + k, 8)], r3.at[g, k - 1], thr_s.at[g], thr_r.at[g], along("z", k)).start()

    def stage_four(g):
        mark(f"four{g}")
        await_recv(r3.at[g], thr_s.at[g], thr_r.at[g])
        v = own2[g, z]
        for k in range(7):
            v = v + r3[g, k].astype(F32)
        fin[g] = v.astype(BF16)
        allf[g, sp] = v.astype(BF16)
        for k in range(1, 16):
            copy(fin.at[g], allf.at[g, sp], fou_s.at[g], fou_r.at[g], {"sp": lax.rem(sp + k, 16), "dp": dp}).start()

    def stage_end(g):
        mark(f"end{g}")
        await_recv(allf.at[g, pl.ds(0, 15)], fou_s.at[g], fou_r.at[g])
        h, n = g // 2, g % 2
        for s in range(16):
            a, b = (s // 4, s % 4) if h == 0 else (s % 4, s // 4)
            wout[h, a * 32:(a + 1) * 32, b * 256 + n * 128:b * 256 + (n + 1) * 128] = allf[g, s]

    far_tiles(0)
    ring(1, 0)
    mix_x()
    stats_pair()
    far_tiles(1)
    near_tiles(0)
    ring(1, 1)
    near_tiles(1)
    help_pair(1)
    own_tiles(0)
    own_tiles(1)
    stats_x()
    for g in range(4):
        relay((0, 2, 1, 3)[g])
    ring(2, 0)
    into(0)
    mix_z()
    into(1)
    stats_y()
    ring(2, 1)
    stage_two(0)
    ring(3, 0)
    stage_two(2)
    mix_y()
    stage_two(1)
    stage_two(3)
    ring(3, 1)
    stats_z()
    for v in range(2):
        help_out(2, v)
    mix_back_z()
    stage_three(0)
    stage_three(2)
    stage_three(1)
    stage_three(3)
    ring(4, 0)
    ring(4, 1)
    for v in range(2):
        help_out(3, v)
        help_out(4, v)
    mark("help_pair2")
    help_pair(2)
    mix_back_x()
    stage_four(0)
    stage_four(2)
    stage_four(1)
    stage_four(3)
    stats_back()
    into(2)
    mark("help_pair3")
    help_pair(3)
    help_pair(4)
    into(3)
    mix_back_c()
    into(4)
    mix_end()
    stats_end()
    for g in (0, 2, 1, 3):
        stage_end(g)

    mark("sends")
    await_send(tokr, tok_s.at[0], tok_r.at[0])
    for h in range(2):
        for j in range(4):
            swap(h, j).wait_send()
    for g in range(4):
        for i in range(6):
            await_send(sup.at[g], one_s.at[g * 6 + i], one_r.at[g * 6 + i])
        await_send(r2.at[g], two_s.at[g], two_r.at[g])
        await_send(r3.at[g], thr_s.at[g], thr_r.at[g])
        await_send(allf.at[g, pl.ds(0, 15)], fou_s.at[g], fou_r.at[g])
    for i, buf in enumerate((mrecv, mr1, mr2, my.at[pl.ds(0, 3)], maz.at[pl.ds(0, 7)],
                             max_.at[pl.ds(0, 3)], mrp)):
        await_send(buf, mix_s.at[i], mix_r.at[i])
    for i, buf in enumerate((stc, stx, sty.at[pl.ds(0, 3)], stz.at[pl.ds(0, 7)], stg.at[pl.ds(0, 3)])):
        await_send(buf, sts_s.at[i], sts_r.at[i])
    for v in range(2):
        await_send(shard[v], pair_s.at[v], pair_r.at[v])
        for h in range(1, 5):
            for d in directions(h, v):
                i = number(d, v, h)
                hop(d, v, h, 0).wait_send()
                hop(d, v, h, 1).wait_send()
                helped(d, v, h).wait_send()
                await_send(top(0, v, 0), pair_s.at[2 + i], pair_r.at[2 + i])
                await_send(low_rows(0, v, 0), pair_s.at[18 + i], pair_r.at[18 + i])
    mark(None)


SCRATCH = (
    pltpu.VMEM((1, 1024), F32),
    pltpu.VMEM((1, 1024), F32),
    pltpu.VMEM((16, 128), F32),
    pltpu.VMEM((384, 1024), BF16),
    pltpu.VMEM((384, 1024), BF16),
    pltpu.VMEM((384, 1024), BF16),
    pltpu.VMEM((16, 128, 128), BF16),
    pltpu.VMEM((8, 384, 128), BF16),
    pltpu.VMEM((8, 128, 256), BF16),
    pltpu.VMEM((8, 128, 256), BF16),
    pltpu.VMEM((384, 1024), F32),
    pltpu.VMEM((384, 1024), F32),
    pltpu.VMEM((384, 1024), BF16),
    pltpu.VMEM((384, 1024), BF16),
    pltpu.VMEM((384, 1024), F32),
    pltpu.VMEM((384, 1024), F32),
    pltpu.VMEM((384, 128), F32),
    pltpu.VMEM((128, 1024), F32),
    pltpu.VMEM((128, 1024), F32),
    pltpu.VMEM((16, 1024), F32),
    pltpu.VMEM((16, 1024), F32),
    pltpu.VMEM((768, 2048), BF16),
    pltpu.VMEM((16, 128, 128), F32),
    pltpu.VMEM((32, 128), F32),
    pltpu.VMEM((8, 384, 128), BF16),
    pltpu.VMEM((1024, 768), BF16),
    pltpu.VMEM((8, 2, 2, 128, 1024), BF16),
    pltpu.VMEM((4, 2, 512, 128), BF16),
    pltpu.VMEM((4, 512, 128), BF16),
    pltpu.VMEM((4, 512, 128), BF16),
    pltpu.VMEM((4, 512, 128), F32),
    pltpu.VMEM((4, 512, 128), F32),
    pltpu.VMEM((4, 2, 512, 128), F32),
    pltpu.VMEM((4, 2, 512, 128), BF16),
    pltpu.VMEM((4, 2, 512, 128), BF16),
    pltpu.VMEM((4, 2, 512, 128), BF16),
    pltpu.VMEM((4, 2, 512, 128), BF16),
    pltpu.VMEM((4, 8, 4, 32, 128), F32),
    pltpu.VMEM((4, 8, 4, 32, 128), BF16),
    pltpu.VMEM((4, 3, 8, 32, 128), BF16),
    pltpu.VMEM((4, 8, 32, 128), F32),
    pltpu.VMEM((4, 8, 32, 128), BF16),
    pltpu.VMEM((4, 7, 32, 128), BF16),
    pltpu.VMEM((4, 32, 128), BF16),
    pltpu.VMEM((4, 16, 32, 128), BF16),
    pltpu.VMEM((8, 128, 128), F32),
    pltpu.VMEM((8, 4, 32, 128), F32),
    pltpu.VMEM((8, 4, 32, 128), BF16),
    pltpu.VMEM((3, 8, 32, 128), BF16),
    pltpu.VMEM((8, 32, 128), F32),
    pltpu.VMEM((8, 32, 128), BF16),
    pltpu.VMEM((7, 32, 128), BF16),
    pltpu.VMEM((4, 32, 128), F32),
    pltpu.VMEM((8, 32, 128), BF16),
    pltpu.VMEM((4, 8, 32, 128), BF16),
    pltpu.VMEM((32, 128), BF16),
    pltpu.VMEM((32, 128), F32),
    pltpu.VMEM((4, 8, 32, 128), BF16),
    pltpu.VMEM((32, 128), F32),
    pltpu.VMEM((3, 8, 128), F32),
    pltpu.VMEM((4, 8, 128), F32),
    pltpu.VMEM((8, 8, 128), F32),
    pltpu.VMEM((4, 8, 128), F32),
    pltpu.VMEM((4, 8, 128), F32),
    pltpu.VMEM((3, 8, 128), F32),
    pltpu.SemaphoreType.DMA((17,)),
    pltpu.SemaphoreType.DMA((1,)), pltpu.SemaphoreType.DMA((1,)),
    pltpu.SemaphoreType.DMA((8,)), pltpu.SemaphoreType.DMA((8,)),
    pltpu.SemaphoreType.DMA((32,)), pltpu.SemaphoreType.DMA((32,)),
    pltpu.SemaphoreType.DMA((16,)), pltpu.SemaphoreType.DMA((16,)),
    pltpu.SemaphoreType.DMA((34,)), pltpu.SemaphoreType.DMA((34,)),
    pltpu.SemaphoreType.DMA((24,)), pltpu.SemaphoreType.DMA((24,)),
    pltpu.SemaphoreType.DMA((4,)), pltpu.SemaphoreType.DMA((4,)),
    pltpu.SemaphoreType.DMA((4,)), pltpu.SemaphoreType.DMA((4,)),
    pltpu.SemaphoreType.DMA((4,)), pltpu.SemaphoreType.DMA((4,)),
    pltpu.SemaphoreType.DMA((7,)), pltpu.SemaphoreType.DMA((7,)),
    pltpu.SemaphoreType.DMA((5,)), pltpu.SemaphoreType.DMA((5,)),
)


def fused_call(tokens, va, ga, cot, vw, gw, mixw, gain, bias, mixb):
    hbm = pl.BlockSpec(memory_space=pltpu.HBM)
    vm = pl.BlockSpec(memory_space=pltpu.VMEM)
    return pl.pallas_call(
        fused,
        out_shape=(
            pltpu.VMEM((384, 2048), BF16),
            pltpu.VMEM((2, 128, 1024), BF16),
            pltpu.VMEM((16, 128, 128), BF16),
            pltpu.VMEM((16, 128), F32),
            pltpu.VMEM((8, 128), F32),
            pltpu.VMEM((8, 128), F32),
        ),
        in_specs=[hbm] * 10,
        out_specs=(vm,) * 6,
        scratch_shapes=list(SCRATCH),
        compiler_params=pltpu.CompilerParams(
            collective_id=0, has_side_effects=True, vmem_limit_bytes=54 * 1024 * 1024),
        name="fused",
    )(tokens, va, ga, cot, vw, gw, mixw, gain, bias, mixb)


def finish(tgrad, wsum, mixs, bsum, nsum, hsum, tout, vout, gout, mout, bout, nout, hout, wide, mwide, osem):
    pairs = [(tgrad, tout), (wide.at[0], vout), (wide.at[1], gout), (mwide, mout), (bsum, bout), (nsum, nout), (hsum, hout)]
    puts = [pltpu.make_async_copy(src, dst, osem.at[k]) for k, (src, dst) in enumerate(pairs)]
    for k in (0, 4, 5, 6):
        puts[k].start()
    for k in range(2):
        wide[k] = wsum[k].astype(F32)
        puts[1 + k].start()
    mwide[...] = mixs[...].astype(F32)
    puts[3].start()
    for put in puts:
        put.wait()


def finish_call(*parts):
    hbm = pl.BlockSpec(memory_space=pltpu.HBM)
    vm = pl.BlockSpec(memory_space=pltpu.VMEM)
    return pl.pallas_call(
        finish,
        out_shape=(
            jax.ShapeDtypeStruct((384, 2048), BF16),
            jax.ShapeDtypeStruct((128, 1024), F32),
            jax.ShapeDtypeStruct((128, 1024), F32),
            jax.ShapeDtypeStruct((16, 128, 128), F32),
            jax.ShapeDtypeStruct((16, 128), F32),
            jax.ShapeDtypeStruct((8, 128), F32),
            jax.ShapeDtypeStruct((8, 128), F32),
        ),
        in_specs=[vm] * 6,
        out_specs=(hbm,) * 7,
        scratch_shapes=[
            pltpu.VMEM((2, 128, 1024), F32),
            pltpu.VMEM((16, 128, 128), F32),
            pltpu.SemaphoreType.DMA((7,)),
        ],
        compiler_params=pltpu.CompilerParams(vmem_limit_bytes=16 * 1024 * 1024),
        name="finish",
    )(*parts)


def shards(tokens, value_act, gate_act, cotangent, value_weight, gate_weight,
           norm_gain, norm_bias, mix_weight, mix_bias):
    parts = fused_call(
        tokens[0], value_act[0], gate_act[0], cotangent[0], value_weight, gate_weight,
        mix_weight, norm_gain[None], norm_bias[None], mix_bias)
    tgrad, vout, gout, mout, bout, nout, hout = finish_call(*parts)
    return tgrad[None], vout, gout, mout, bout, nout.reshape(1024), hout.reshape(1024)


def solution(mesh):
    rows = P("dp", "sp", None)
    placed = (rows, rows, rows, rows, P("dp", None), P("dp", None), P(), P(), P(), P())
    return jax.shard_map(
        shards, mesh=mesh, in_specs=placed,
        out_specs=(rows, P("dp", None), P("dp", None), P(), P(), P(), P()), check_vma=False)
```

```python
import functools
import jax
import jax.numpy as jnp
from jax import lax
from jax.experimental import pallas as pl
from jax.experimental.pallas import tpu as pltpu
from jax.sharding import PartitionSpec as P

EPSILON = 1e-06
F32, BF16 = jnp.float32, jnp.bfloat16
NT = (((1,), (1,)), ((), ()))
TN = (((0,), (0,)), ((), ()))
NN = (((1,), (0,)), ((), ()))


TOP = 96
GATE_UNROLL = 4
LAST_UNROLL = 4
PROFILE = False
_open = []


def mark(name):
    if not PROFILE:
        return
    while _open:
        _open.pop().__exit__(None, None, None)
    if name:
        scope = jax.named_scope(name)
        scope.__enter__()
        _open.append(scope)


def dot(a, b, dims=NN):
    return lax.dot_general(a, b, dims, preferred_element_type=F32)


def split3(v):
    hi = v.astype(BF16)
    rest = v - hi.astype(F32)
    mid = rest.astype(BF16)
    low = (rest - mid.astype(F32)).astype(BF16)
    return hi, mid, low


def phi_terms(v):
    cdf = 0.5 * (1.0 + lax.erf(v * 0.7071067811865476))
    pdf = jnp.exp(-0.5 * v * v) * 0.3989422804014327
    return cdf, cdf + v * pdf


def fused(tokens, va_h, ga_h, cot_h, vw, gw, mixw_h, gain_h, bias_h, mixb_h,
          tgrad, wout, mixo, bout, nout, hout, gain, bias, mixb,
          va, ga, cot, mixw, tokl, mcat, mtrn, normed, slope, spread, low, cv, gnorm, inv, gsum, bfull, acc_g, acc_b,
          grads, wgrad, stats,
          tokr, tt, wbuf,
          sfar, sup, sdn, fup, fdn, own1, agg, rlay, rprev, rnext, s1f, s1b, r2, own2, s2b, r3, fin, allf,
          mrecv, mq, mqb, mr1, mq1, mq1b, mr2, my, maz, max_, macc, mpart, mrp,
          stc, stx, sty, stz, stg, st0, st1,
          loc, tok_s, tok_r, grd_s, grd_r, ring_s, ring_r, help_s, help_r, pair_s, pair_r, one_s, one_r, two_s, two_r,
          thr_s, thr_r, fou_s, fou_r, mix_s, mix_r, sts_s, sts_r):
    sp = lax.axis_index("sp")
    dp = lax.axis_index("dp")
    y, x = sp // 4, lax.rem(sp, 4)
    z, c = dp // 2, lax.rem(dp, 2)
    pc = 1 - c

    def at(nx=None, ny=None, nz=None, nc=None):
        nx = x if nx is None else nx
        ny = y if ny is None else ny
        nz = z if nz is None else nz
        nc = c if nc is None else nc
        return {"sp": ny * 4 + nx, "dp": nz * 2 + nc}

    def along(axis, k):
        if axis == "x":
            return at(nx=lax.rem(x + k, 4))
        if axis == "y":
            return at(ny=lax.rem(y + k, 4))
        return at(nz=lax.rem(z + k, 8))

    def copy(src, dst, ssem, rsem, to):
        return pltpu.make_async_remote_copy(
            src_ref=src, dst_ref=dst, send_sem=ssem, recv_sem=rsem,
            device_id=to, device_id_type=pl.DeviceIdType.MESH)

    def await_recv(dst, ssem, rsem):
        copy(dst, dst, ssem, rsem, at(nc=pc)).wait_recv()

    def await_send(src, ssem, rsem):
        copy(src, src, ssem, rsem, at(nc=pc)).wait_send()


    mark("barrier")
    barrier = pltpu.get_barrier_semaphore()
    pl.semaphore_signal(barrier, inc=1, device_id=at(nc=pc), device_id_type=pl.DeviceIdType.MESH)
    for k in range(1, 8):
        pl.semaphore_signal(barrier, inc=1, device_id=along("z", k), device_id_type=pl.DeviceIdType.MESH)
    for k in range(1, 16):
        pl.semaphore_signal(barrier, inc=1, device_id={"sp": lax.rem(sp + k, 16), "dp": dp},
                            device_id_type=pl.DeviceIdType.MESH)
    shard = (vw, gw)
    local = [pltpu.make_async_copy(va_h, va, loc.at[0]), pltpu.make_async_copy(cot_h, cot, loc.at[1]),
             pltpu.make_async_copy(ga_h, ga, loc.at[2])]
    for v in range(2):
        local.append(pltpu.make_async_copy(shard[v], wbuf.at[z, v, c], loc.at[3 + v]))
    for k in range(8):
        lanes = pl.ds(pl.multiple_of((2 * k + c) * 128, 128), 128)
        local.append(pltpu.make_async_copy(tokens.at[:, lanes], tokl.at[k], loc.at[5 + k]))
    local.append(pltpu.make_async_copy(mixw_h, mixw, loc.at[13]))
    local.append(pltpu.make_async_copy(gain_h, gain, loc.at[14]))
    local.append(pltpu.make_async_copy(bias_h, bias, loc.at[15]))
    local.append(pltpu.make_async_copy(mixb_h, mixb, loc.at[16]))
    for n in (13, 16, 0, 1, 2, 14, 15, 5, 6, 7, 8, 9, 10, 11, 12, 3, 4):
        local[n].start()

    axes = ("x", "y")
    place = (x, y)

    def top(zz, v, cc):
        return wbuf.at[zz, v, cc, pl.ds(0, TOP)]

    def low_rows(zz, v, cc):
        return wbuf.at[zz, v, cc, pl.ds(TOP, 128 - TOP)]

    def slice_of(zz, v, cc):
        return wbuf.at[zz, v, cc, pl.ds(TOP, 128 - TOP), pl.ds(pl.multiple_of(place[v] * 256, 256), 256)]

    def came_from(direction, h):
        return lax.rem(z - h + 8, 8) if direction == 0 else lax.rem(z + h, 8)

    def last_hop(direction, v):
        return 4 if direction == v else 3

    def number(direction, v, h):
        return (direction * 2 + v) * 4 + h - 1

    def hop(direction, v, h, part):
        origin = came_from(direction, h - 1)
        dst = (top, slice_of)[part](origin, v, c)
        if h > 1:
            src = dst
        elif part == 0:
            src = shard[v].at[pl.ds(0, TOP)]
        else:
            src = shard[v].at[pl.ds(TOP, 128 - TOP), pl.ds(pl.multiple_of(place[v] * 256, 256), 256)]
        i = number(direction, v, h) + 16 * part
        return copy(src, dst, ring_s.at[i], ring_r.at[i], along("z", 1 if direction == 0 else 7))

    def directions(h, v):
        return [d for d in range(2) if h <= last_hop(d, v)]

    def ring_part(h, v, part):
        for d in directions(h, v):
            hop(d, v, h, part).wait_recv()
            if h < last_hop(d, v):
                hop(d, v, h + 1, part).start()

    def ring_step(h, v):
        if h > 1:
            ring_part(h, v, 1)
        ring_part(h, v, 0)
        for d in directions(h, v):
            ref = top(came_from(d, h), v, c)
            i = 2 + number(d, v, h)
            copy(ref, ref, pair_s.at[i], pair_r.at[i], at(nc=pc)).start()

    def help_out(h, v):
        for d in directions(h, v):
            i = number(d, v, h)
            ref = slice_of(came_from(d, h), v, c)
            for k in range(1, 4):
                copy(ref, ref, help_s.at[i], help_r.at[i], along(axes[v], k)).start()

    def helped(d, v, h):
        ref = wbuf.at[0, v, 0, pl.ds(TOP, 128 - TOP), pl.ds(0, 768)]
        return copy(ref, ref, help_s.at[number(d, v, h)], help_r.at[number(d, v, h)], at(nc=pc))

    def help_pair(h):
        for v in range(2):
            for d in directions(h, v):
                helped(d, v, h).wait_recv()
                ref = low_rows(came_from(d, h), v, c)
                i = 18 + number(d, v, h)
                copy(ref, ref, pair_s.at[i], pair_r.at[i], at(nc=pc)).start()

    def await_pair(h):
        for v in range(2):
            if h == 0:
                await_recv(wbuf.at[0, v, 0], pair_s.at[v], pair_r.at[v])
                continue
            for d in directions(h, v):
                i = number(d, v, h)
                await_recv(top(0, v, 0), pair_s.at[2 + i], pair_r.at[2 + i])
                await_recv(low_rows(0, v, 0), pair_s.at[18 + i], pair_r.at[18 + i])

    def into_tokens(zz):
        wv = wbuf[zz, 0].reshape(256, 1024)
        wg = wbuf[zz, 1].reshape(256, 1024)
        out = dot(grads[0:384, 0:1024], wv, NT) + dot(grads[0:384, 1024:2048], wg, NT)
        tgrad[:, pl.ds(pl.multiple_of(zz * 256, 256), 256)] = out.astype(BF16)

    rows = 16
    row = lax.broadcasted_iota(jnp.int32, (128, 128), 0)
    col = lax.broadcasted_iota(jnp.int32, (128, 128), 1)
    keep = row >= col

    gsum[...] = jnp.zeros_like(gsum)
    acc_g[...] = jnp.zeros_like(acc_g)
    acc_b[...] = jnp.zeros_like(acc_b)
    mark("m_prep")
    local[13].wait()
    def prep(p, _):
        for h in range(2):
            m = jnp.where(keep, mixw[2 * p + h].astype(F32), 0.0)
            mcat[p, :, h * 128:(h + 1) * 128] = m.astype(BF16)
            mtrn[p, :, h * 128:(h + 1) * 128] = m.T.astype(BF16)
        return 0

    lax.fori_loop(0, 8, prep, 0)
    group = lax.broadcasted_iota(jnp.int32, (16, 1024), 0)
    chan = lax.broadcasted_iota(jnp.int32, (16, 1024), 1) // 64
    pick = jnp.where(group == chan, 1.0, 0.0).astype(BF16)
    local[16].wait()
    parts = split3(mixb[...])
    bfull[...] = dot(parts[0], pick, TN) + dot(parts[1], pick, TN) + dot(parts[2], pick, TN)

    mark("barrierwait")
    pl.semaphore_wait(barrier, 23)
    for part in (1, 0):
        for v in range(2):
            for direction in range(2):
                hop(direction, v, 1, part).start()
    for k in range(8):
        lanes = pl.ds(pl.multiple_of((2 * k + pc) * 128, 128), 128)
        copy(tokens.at[:, lanes], tokr.at[k], tok_s.at[0], tok_r.at[0], at(nc=pc)).start()
    for v in range(2):
        copy(shard[v], wbuf.at[z, v, c], pair_s.at[v], pair_r.at[v], at(nc=pc)).start()

    mark("m_value")
    local[0].wait()
    local[1].wait()
    def first(i, _):
        at = pl.ds(pl.multiple_of(i * rows, rows), rows)
        v = va[at, :].astype(F32)
        cdf, slp = phi_terms(v)
        c = cot[at, :].astype(F32)
        gs = c * (v * cdf)
        low[at, :] = gs.astype(BF16)
        cv[at, :] = c * slp
        inb = pl.ds(pl.multiple_of(lax.rem(i, 8) * rows, rows), rows)
        gsum[inb, :] += gs
        return 0

    lax.fori_loop(0, 24, first, 0)

    mark("m_gate")
    local[2].wait()
    local[14].wait()
    local[15].wait()
    def second(i, _):
        for u in range(GATE_UNROLL):
            rat = pl.ds(pl.multiple_of((i * GATE_UNROLL + u) * rows, rows), rows)
            v = ga[rat, :].astype(F32)
            cdf, slp = phi_terms(v)
            slope[rat, :] = slp
            g = v * cdf
            cen = g - jnp.mean(g, axis=-1, keepdims=True)
            s = lax.rsqrt(jnp.mean(cen * cen, axis=-1, keepdims=True) + EPSILON)
            n = cen * s
            normed[rat, :] = n
            inv[rat, :] = jnp.broadcast_to(s, (rows, 128))
            spread[rat, :] = (n * gain[...] + bias[...]).astype(BF16)
        return 0

    lax.fori_loop(0, 24 // GATE_UNROLL, second, 0)

    mark("help1")
    for v in range(2):
        ring_part(1, v, 1)
        help_out(1, v)
    mark("m_mix")
    lane = lax.broadcasted_iota(jnp.int32, (1, 128), 1)
    m0 = jnp.where(lane < 64, 1.0, 0.0).astype(BF16)
    m1 = jnp.where(lane < 64, 0.0, 1.0).astype(BF16)

    def mix_pair(p):
        cols = pl.ds(pl.multiple_of(p * 128, 128), 128)
        wg = None
        for b in range(3):
            r = slice(b * 128, (b + 1) * 128)
            s = spread[r, cols]
            l = low[r, cols]
            stack_s = jnp.concatenate((s * m0, s * m1), axis=0)
            stack_l = jnp.concatenate((l * m0, l * m1), axis=0)
            spatial = dot(mcat[p], stack_s) + bfull[:, cols]
            grads[r, cols] = (cv[r, cols] * spatial).astype(BF16)
            gnorm[r, cols] = dot(mtrn[p], stack_l)
            term = dot(stack_l, s, NT)
            wg = term if wg is None else wg + term
        wgrad[2 * p] = jnp.where(keep, wg[:128], 0.0)
        wgrad[2 * p + 1] = jnp.where(keep, wg[128:], 0.0)

    reach = (2, 1, 3, 0)

    def swap(h, j):
        dest = lax.rem(place[h] + reach[j], 4)
        lanes = pl.ds(pl.multiple_of(h * 1024 + dest * 256, 256), 256)
        return copy(grads.at[pl.ds(0, 384), lanes], grads.at[pl.ds(384, 384), lanes],
                    grd_s.at[h * 4 + j], grd_r.at[h * 4 + j], at(nc=pc))

    def mix(j, _):
        dest = lax.rem(x + 2 + j, 4)
        mix_pair(2 * dest)
        mix_pair(2 * dest + 1)
        return 0

    mix(0, 0)
    swap(0, 0).start()
    lax.fori_loop(1, 4, mix, 0)
    for j in (1, 2, 3):
        swap(0, j).start()
    for k in range(8):
        copy(wgrad.at[2 * k + pc], mrecv.at[k], mix_s.at[0], mix_r.at[0], at(nc=pc)).start()

    mark("m_last")
    def last(i, _):
        for u in range(LAST_UNROLL):
            rat = pl.ds(pl.multiple_of((i * LAST_UNROLL + u) * rows, rows), rows)
            gn = gnorm[rat, :]
            n = normed[rat, :]
            gnn = gn * n
            acc_g[...] += gnn
            acc_b[...] += gn
            h = gn * gain[...]
            mean_h = jnp.mean(h, axis=-1, keepdims=True)
            mean_hn = jnp.mean(h * n, axis=-1, keepdims=True)
            s = inv[rat, 0:1]
            out = s * (h - mean_h - n * mean_hn)
            grads[rat, 1024:2048] = (out * slope[rat, :]).astype(BF16)
        return 0

    lax.fori_loop(0, 24 // LAST_UNROLL, last, 0)
    for j in range(4):
        swap(1, j).start()
    mark("transpose")
    for k in range(8):
        local[5 + k].wait()
        tt[k * 128:(k + 1) * 128, 0:384] = tokl[k].T
    await_recv(tokr, tok_s.at[0], tok_r.at[0])
    for k in range(8):
        tt[k * 128:(k + 1) * 128, 384:768] = tokr[k].T
    def stats_pair():
        mark("m_stats")
        parts = split3(gsum[...])
        stats[0:16, :] = dot(pick, parts[0], NT) + dot(pick, parts[1], NT) + dot(pick, parts[2], NT)
        tot_g = jnp.sum(acc_g[...], axis=0, keepdims=True)
        tot_b = jnp.sum(acc_b[...], axis=0, keepdims=True)
        for k in range(8):
            stats[16 + k:17 + k, :] = tot_g[:, k * 128:(k + 1) * 128]
            stats[24 + k:25 + k, :] = tot_b[:, k * 128:(k + 1) * 128]
        copy(stats, stc, sts_s.at[0], sts_r.at[0], at(nc=pc)).start()

    def product(h, j, half):
        swap_in(h, j)
        dest = lax.rem(place[h] + reach[j], 4)
        wide = pl.ds(pl.multiple_of(h * 1024 + dest * 256, 256), 256)
        v = dot(tt[half * 512:(half + 1) * 512, :], grads[:, wide])
        return v[:, :128], v[:, 128:]

    arrived = set()

    def swap_in(h, j):
        if (h, j) not in arrived:
            arrived.add((h, j))
            swap(h, j).wait_recv()

    def one(i, g, src, dst, k):
        return copy(src, dst, one_s.at[g * 6 + i], one_r.at[g * 6 + i], along(axes[g // 2], k))

    def far_tiles(h):
        mark(f"far{h}")
        for half, k in ((0, 1), (1, 3)):
            v = product(h, 0, half)
            for n in range(2):
                g = 2 * h + n
                sfar[g, half] = v[n].astype(BF16)
                one(half, g, sfar.at[g, half], rlay.at[g, half], k).start()

    def near_tiles(h):
        mark(f"near{h}")
        v = product(h, 1, 1)
        for n in range(2):
            g = 2 * h + n
            sup[g] = v[n].astype(BF16)
            one(2, g, sup.at[g], rprev.at[g, 1], 1).start()
        v = product(h, 2, 0)
        for n in range(2):
            g = 2 * h + n
            sdn[g] = v[n].astype(BF16)
            one(3, g, sdn.at[g], rnext.at[g, 0], 3).start()
        fup[2 * h], fup[2 * h + 1] = product(h, 1, 0)
        fdn[2 * h], fdn[2 * h + 1] = product(h, 2, 1)

    def own_tiles(h):
        mark(f"own{h}")
        for half in range(2):
            own1[2 * h, half], own1[2 * h + 1, half] = product(h, 3, half)

    def relay(g):
        mark(f"relay{g}")
        one(0, g, rlay.at[g, 0], rlay.at[g, 0], 1).wait_recv()
        agg[g, 0] = (fup[g] + rlay[g, 0].astype(F32)).astype(BF16)
        one(4, g, agg.at[g, 0], rprev.at[g, 0], 1).start()
        one(1, g, rlay.at[g, 1], rlay.at[g, 1], 3).wait_recv()
        agg[g, 1] = (fdn[g] + rlay[g, 1].astype(F32)).astype(BF16)
        one(5, g, agg.at[g, 1], rnext.at[g, 1], 3).start()

    def stats_x():
        mark("stats_x")
        await_recv(stc, sts_s.at[0], sts_r.at[0])
        st0[...] = (stats[...] + stc[...]).reshape(4, 8, 128)
        for k in range(1, 4):
            copy(st0.at[lax.rem(x + k, 4)], stx.at[k - 1], sts_s.at[1], sts_r.at[1], along("x", k)).start()

    def stats_y():
        mark("stats_y")
        await_recv(stx, sts_s.at[1], sts_r.at[1])
        st1[0] = ((st0[x] + stx[0]) + stx[1]) + stx[2]
        sty[y] = st1[0]
        for k in range(1, 4):
            copy(st1.at[0], sty.at[y], sts_s.at[2], sts_r.at[2], along("y", k)).start()

    def stats_z():
        mark("stats_z")
        await_recv(sty.at[pl.ds(0, 3)], sts_s.at[2], sts_r.at[2])
        st1[1] = (sty[0] + sty[1]) + (sty[2] + sty[3])
        stz[z] = st1[1]
        for k in range(1, 8):
            copy(st1.at[1], stz.at[z], sts_s.at[3], sts_r.at[3], along("z", k)).start()

    def stats_back():
        mark("stats_back")
        await_recv(stz.at[pl.ds(0, 7)], sts_s.at[3], sts_r.at[3])
        t = stz[0]
        for k in range(1, 8):
            t = t + stz[k]
        st1[2] = t
        stg[x] = t
        for k in range(1, 4):
            copy(st1.at[2], stg.at[x], sts_s.at[4], sts_r.at[4], along("x", k)).start()

    def stats_end():
        mark("stats_end")
        await_recv(stg.at[pl.ds(0, 3)], sts_s.at[4], sts_r.at[4])
        bout[0:8] = stg[0]
        bout[8:16] = stg[1]
        nout[...] = stg[2]
        hout[...] = stg[3]

    def mix_x():
        mark("mix_x")
        await_recv(mrecv, mix_s.at[0], mix_r.at[0])
        for k in range(8):
            v = (wgrad[2 * k + c] + mrecv[k]).reshape(4, 32, 128)
            mq[k] = v
            mqb[k] = v.astype(BF16)
        for k in range(1, 4):
            for h in range(2):
                copy(mqb.at[pl.ds(4 * h, 4), lax.rem(place[h] + k, 4)], mr1.at[k - 1, pl.ds(4 * h, 4)],
                     mix_s.at[1], mix_r.at[1], along(axes[h], k)).start()

    def mix_z():
        mark("mix_z")
        await_recv(mr1, mix_s.at[1], mix_r.at[1])
        for h in range(2):
            r = slice(4 * h, 4 * h + 4)
            v = mq[r, place[h]] + (mr1[0, r].astype(F32) + mr1[1, r].astype(F32)) + mr1[2, r].astype(F32)
            mq1[r] = v
            mq1b[r] = v.astype(BF16)
        for k in range(1, 8):
            copy(mq1b.at[lax.rem(z + k, 8)], mr2.at[k - 1], mix_s.at[2], mix_r.at[2], along("z", k)).start()

    def mix_y():
        mark("mix_y")
        await_recv(mr2, mix_s.at[2], mix_r.at[2])
        v = mq1[z]
        for k in range(7):
            v = v + mr2[k].astype(F32)
        mpart[...] = v
        on_x = z // 4
        slot = y * (1 - on_x) + x * on_x
        my[slot] = v
        for k in range(1, 4):
            to = at(nx=lax.rem(x + k * on_x, 4), ny=lax.rem(y + k * (1 - on_x), 4))
            copy(mpart, my.at[slot], mix_s.at[3], mix_r.at[3], to).start()

    def mix_back_z():
        mark("mix_back_z")
        await_recv(my.at[pl.ds(0, 3)], mix_s.at[3], mix_r.at[3])
        v = ((my[0] + my[1]) + (my[2] + my[3])).astype(BF16)
        macc[...] = v
        maz[z] = v
        for k in range(1, 8):
            copy(macc, maz.at[z], mix_s.at[4], mix_r.at[4], along("z", k)).start()

    def mix_back_x():
        mark("mix_back_x")
        await_recv(maz.at[pl.ds(0, 7)], mix_s.at[4], mix_r.at[4])
        for h in range(2):
            r = pl.ds(4 * h, 4)
            max_[place[h], r] = maz[r]
            for k in range(1, 4):
                copy(maz.at[r], max_.at[place[h], r], mix_s.at[5], mix_r.at[5], along(axes[h], k)).start()

    def mix_back_c():
        mark("mix_back_c")
        await_recv(max_.at[pl.ds(0, 3)], mix_s.at[5], mix_r.at[5])
        copy(max_, mrp, mix_s.at[6], mix_r.at[6], at(nc=pc)).start()

    def mix_end():
        mark("mix_end")
        await_recv(mrp, mix_s.at[6], mix_r.at[6])
        for k in range(8):
            mixo[2 * k + c] = max_[:, k].reshape(128, 128)
            mixo[2 * k + pc] = mrp[:, k].reshape(128, 128)

    def ring(h, v):
        mark(f"ring{h}{v}")
        ring_step(h, v)

    def into(h):
        mark(f"into{h}")
        await_pair(h)
        if h == 0:
            local[3].wait()
            local[4].wait()
            into_tokens(z)
            return
        into_tokens(lax.rem(z + h, 8))
        if h < 4:
            into_tokens(lax.rem(z + 8 - h, 8))

    def stage_two(g):
        mark(f"two{g}")
        for i, buf in ((2, rprev.at[g, 1]), (3, rnext.at[g, 0]), (4, rprev.at[g, 0]), (5, rnext.at[g, 1])):
            one(i, g, buf, buf, 1).wait_recv()
        for q in range(2):
            v = own1[g, q] + (rprev[g, q].astype(F32) + rnext[g, q].astype(F32))
            v = v.reshape(4, 4, 32, 128)
            s1f[g, 4 * q:4 * q + 4] = v
            s1b[g, 4 * q:4 * q + 4] = v.astype(BF16)
        h = g // 2
        other = place[1 - h]
        for k in (2, 1, 3):
            copy(s1b.at[g, :, lax.rem(other + k, 4)], r2.at[g, k - 1], two_s.at[g], two_r.at[g],
                 along(axes[1 - h], k)).start()

    def stage_three(g):
        mark(f"three{g}")
        await_recv(r2.at[g], two_s.at[g], two_r.at[g])
        v = s1f[g, :, place[1 - g // 2]] + (r2[g, 0].astype(F32) + r2[g, 1].astype(F32)) + r2[g, 2].astype(F32)
        own2[g] = v
        s2b[g] = v.astype(BF16)
        for k in (4, 3, 5, 2, 6, 1, 7):
            copy(s2b.at[g, lax.rem(z + k, 8)], r3.at[g, k - 1], thr_s.at[g], thr_r.at[g], along("z", k)).start()

    def stage_four(g):
        mark(f"four{g}")
        await_recv(r3.at[g], thr_s.at[g], thr_r.at[g])
        v = own2[g, z]
        for k in range(7):
            v = v + r3[g, k].astype(F32)
        fin[g] = v.astype(BF16)
        allf[g, sp] = v.astype(BF16)
        for k in (10, 6, 9, 11, 14, 2, 5, 7, 8, 13, 15, 1, 3, 4, 12):
            copy(fin.at[g], allf.at[g, sp], fou_s.at[g], fou_r.at[g], {"sp": lax.rem(sp + k, 16), "dp": dp}).start()

    def stage_end(g):
        mark(f"end{g}")
        await_recv(allf.at[g, pl.ds(0, 15)], fou_s.at[g], fou_r.at[g])
        h, n = g // 2, g % 2
        for s in range(16):
            a, b = (s // 4, s % 4) if h == 0 else (s % 4, s // 4)
            wout[h, a * 32:(a + 1) * 32, b * 256 + n * 128:b * 256 + (n + 1) * 128] = allf[g, s]

    far_tiles(0)
    far_tiles(1)
    ring(1, 0)
    mix_x()
    stats_pair()
    near_tiles(0)
    ring(1, 1)
    near_tiles(1)
    help_pair(1)
    own_tiles(0)
    own_tiles(1)
    stats_x()
    for g in range(4):
        relay((0, 2, 1, 3)[g])
    ring(2, 0)
    into(0)
    mix_z()
    into(1)
    ring(2, 1)
    stage_two(0)
    ring(3, 0)
    stage_two(2)
    mix_y()
    stage_two(1)
    stage_two(3)
    stats_y()
    ring(3, 1)
    for v in range(2):
        help_out(2, v)
    mix_back_z()
    stage_three(0)
    stage_three(2)
    stage_three(1)
    stage_three(3)
    stats_z()
    ring(4, 0)
    ring(4, 1)
    for v in range(2):
        help_out(3, v)
        help_out(4, v)
    mark("help_pair2")
    help_pair(2)
    mix_back_x()
    stage_four(0)
    stage_four(2)
    stage_four(1)
    stage_four(3)
    mark("help_pair3")
    help_pair(3)
    help_pair(4)
    into(2)
    stats_back()
    into(3)
    mix_back_c()
    into(4)
    mix_end()
    stats_end()
    for g in (0, 2, 1, 3):
        stage_end(g)

    mark("sends")
    await_send(tokr, tok_s.at[0], tok_r.at[0])
    for h in range(2):
        for j in range(4):
            swap(h, j).wait_send()
    for g in range(4):
        for i in range(6):
            await_send(sup.at[g], one_s.at[g * 6 + i], one_r.at[g * 6 + i])
        await_send(r2.at[g], two_s.at[g], two_r.at[g])
        await_send(r3.at[g], thr_s.at[g], thr_r.at[g])
        await_send(allf.at[g, pl.ds(0, 15)], fou_s.at[g], fou_r.at[g])
    for i, buf in enumerate((mrecv, mr1, mr2, my.at[pl.ds(0, 3)], maz.at[pl.ds(0, 7)],
                             max_.at[pl.ds(0, 3)], mrp)):
        await_send(buf, mix_s.at[i], mix_r.at[i])
    for i, buf in enumerate((stc, stx, sty.at[pl.ds(0, 3)], stz.at[pl.ds(0, 7)], stg.at[pl.ds(0, 3)])):
        await_send(buf, sts_s.at[i], sts_r.at[i])
    for v in range(2):
        await_send(shard[v], pair_s.at[v], pair_r.at[v])
        for h in range(1, 5):
            for d in directions(h, v):
                i = number(d, v, h)
                hop(d, v, h, 0).wait_send()
                hop(d, v, h, 1).wait_send()
                helped(d, v, h).wait_send()
                await_send(top(0, v, 0), pair_s.at[2 + i], pair_r.at[2 + i])
                await_send(low_rows(0, v, 0), pair_s.at[18 + i], pair_r.at[18 + i])
    mark(None)


SCRATCH = (
    pltpu.VMEM((1, 1024), F32),
    pltpu.VMEM((1, 1024), F32),
    pltpu.VMEM((16, 128), F32),
    pltpu.VMEM((384, 1024), BF16),
    pltpu.VMEM((384, 1024), BF16),
    pltpu.VMEM((384, 1024), BF16),
    pltpu.VMEM((16, 128, 128), BF16),
    pltpu.VMEM((8, 384, 128), BF16),
    pltpu.VMEM((8, 128, 256), BF16),
    pltpu.VMEM((8, 128, 256), BF16),
    pltpu.VMEM((384, 1024), F32),
    pltpu.VMEM((384, 1024), F32),
    pltpu.VMEM((384, 1024), BF16),
    pltpu.VMEM((384, 1024), BF16),
    pltpu.VMEM((384, 1024), F32),
    pltpu.VMEM((384, 1024), F32),
    pltpu.VMEM((384, 128), F32),
    pltpu.VMEM((128, 1024), F32),
    pltpu.VMEM((128, 1024), F32),
    pltpu.VMEM((16, 1024), F32),
    pltpu.VMEM((16, 1024), F32),
    pltpu.VMEM((768, 2048), BF16),
    pltpu.VMEM((16, 128, 128), F32),
    pltpu.VMEM((32, 128), F32),
    pltpu.VMEM((8, 384, 128), BF16),
    pltpu.VMEM((1024, 768), BF16),
    pltpu.VMEM((8, 2, 2, 128, 1024), BF16),
    pltpu.VMEM((4, 2, 512, 128), BF16),
    pltpu.VMEM((4, 512, 128), BF16),
    pltpu.VMEM((4, 512, 128), BF16),
    pltpu.VMEM((4, 512, 128), F32),
    pltpu.VMEM((4, 512, 128), F32),
    pltpu.VMEM((4, 2, 512, 128), F32),
    pltpu.VMEM((4, 2, 512, 128), BF16),
    pltpu.VMEM((4, 2, 512, 128), BF16),
    pltpu.VMEM((4, 2, 512, 128), BF16),
    pltpu.VMEM((4, 2, 512, 128), BF16),
    pltpu.VMEM((4, 8, 4, 32, 128), F32),
    pltpu.VMEM((4, 8, 4, 32, 128), BF16),
    pltpu.VMEM((4, 3, 8, 32, 128), BF16),
    pltpu.VMEM((4, 8, 32, 128), F32),
    pltpu.VMEM((4, 8, 32, 128), BF16),
    pltpu.VMEM((4, 7, 32, 128), BF16),
    pltpu.VMEM((4, 32, 128), BF16),
    pltpu.VMEM((4, 16, 32, 128), BF16),
    pltpu.VMEM((8, 128, 128), F32),
    pltpu.VMEM((8, 4, 32, 128), F32),
    pltpu.VMEM((8, 4, 32, 128), BF16),
    pltpu.VMEM((3, 8, 32, 128), BF16),
    pltpu.VMEM((8, 32, 128), F32),
    pltpu.VMEM((8, 32, 128), BF16),
    pltpu.VMEM((7, 32, 128), BF16),
    pltpu.VMEM((4, 32, 128), F32),
    pltpu.VMEM((8, 32, 128), BF16),
    pltpu.VMEM((4, 8, 32, 128), BF16),
    pltpu.VMEM((32, 128), BF16),
    pltpu.VMEM((32, 128), F32),
    pltpu.VMEM((4, 8, 32, 128), BF16),
    pltpu.VMEM((32, 128), F32),
    pltpu.VMEM((3, 8, 128), F32),
    pltpu.VMEM((4, 8, 128), F32),
    pltpu.VMEM((8, 8, 128), F32),
    pltpu.VMEM((4, 8, 128), F32),
    pltpu.VMEM((4, 8, 128), F32),
    pltpu.VMEM((3, 8, 128), F32),
    pltpu.SemaphoreType.DMA((17,)),
    pltpu.SemaphoreType.DMA((1,)), pltpu.SemaphoreType.DMA((1,)),
    pltpu.SemaphoreType.DMA((8,)), pltpu.SemaphoreType.DMA((8,)),
    pltpu.SemaphoreType.DMA((32,)), pltpu.SemaphoreType.DMA((32,)),
    pltpu.SemaphoreType.DMA((16,)), pltpu.SemaphoreType.DMA((16,)),
    pltpu.SemaphoreType.DMA((34,)), pltpu.SemaphoreType.DMA((34,)),
    pltpu.SemaphoreType.DMA((24,)), pltpu.SemaphoreType.DMA((24,)),
    pltpu.SemaphoreType.DMA((4,)), pltpu.SemaphoreType.DMA((4,)),
    pltpu.SemaphoreType.DMA((4,)), pltpu.SemaphoreType.DMA((4,)),
    pltpu.SemaphoreType.DMA((4,)), pltpu.SemaphoreType.DMA((4,)),
    pltpu.SemaphoreType.DMA((7,)), pltpu.SemaphoreType.DMA((7,)),
    pltpu.SemaphoreType.DMA((5,)), pltpu.SemaphoreType.DMA((5,)),
)


def fused_call(tokens, va, ga, cot, vw, gw, mixw, gain, bias, mixb):
    hbm = pl.BlockSpec(memory_space=pltpu.HBM)
    vm = pl.BlockSpec(memory_space=pltpu.VMEM)
    return pl.pallas_call(
        fused,
        out_shape=(
            pltpu.VMEM((384, 2048), BF16),
            pltpu.VMEM((2, 128, 1024), BF16),
            pltpu.VMEM((16, 128, 128), BF16),
            pltpu.VMEM((16, 128), F32),
            pltpu.VMEM((8, 128), F32),
            pltpu.VMEM((8, 128), F32),
        ),
        in_specs=[hbm] * 10,
        out_specs=(vm,) * 6,
        scratch_shapes=list(SCRATCH),
        compiler_params=pltpu.CompilerParams(
            collective_id=0, has_side_effects=True, vmem_limit_bytes=54 * 1024 * 1024),
        name="fused",
    )(tokens, va, ga, cot, vw, gw, mixw, gain, bias, mixb)


def finish(tgrad, wsum, mixs, bsum, nsum, hsum, tout, vout, gout, mout, bout, nout, hout, wide, mwide, osem):
    pairs = [(tgrad, tout), (wide.at[0], vout), (wide.at[1], gout), (mwide, mout), (bsum, bout), (nsum, nout), (hsum, hout)]
    puts = [pltpu.make_async_copy(src, dst, osem.at[k]) for k, (src, dst) in enumerate(pairs)]
    for k in (0, 4, 5, 6):
        puts[k].start()
    for k in range(2):
        wide[k] = wsum[k].astype(F32)
        puts[1 + k].start()
    mwide[...] = mixs[...].astype(F32)
    puts[3].start()
    for put in puts:
        put.wait()


def finish_call(*parts):
    hbm = pl.BlockSpec(memory_space=pltpu.HBM)
    vm = pl.BlockSpec(memory_space=pltpu.VMEM)
    return pl.pallas_call(
        finish,
        out_shape=(
            jax.ShapeDtypeStruct((384, 2048), BF16),
            jax.ShapeDtypeStruct((128, 1024), F32),
            jax.ShapeDtypeStruct((128, 1024), F32),
            jax.ShapeDtypeStruct((16, 128, 128), F32),
            jax.ShapeDtypeStruct((16, 128), F32),
            jax.ShapeDtypeStruct((8, 128), F32),
            jax.ShapeDtypeStruct((8, 128), F32),
        ),
        in_specs=[vm] * 6,
        out_specs=(hbm,) * 7,
        scratch_shapes=[
            pltpu.VMEM((2, 128, 1024), F32),
            pltpu.VMEM((16, 128, 128), F32),
            pltpu.SemaphoreType.DMA((7,)),
        ],
        compiler_params=pltpu.CompilerParams(vmem_limit_bytes=16 * 1024 * 1024),
        name="finish",
    )(*parts)


def shards(tokens, value_act, gate_act, cotangent, value_weight, gate_weight,
           norm_gain, norm_bias, mix_weight, mix_bias):
    parts = fused_call(
        tokens[0], value_act[0], gate_act[0], cotangent[0], value_weight, gate_weight,
        mix_weight, norm_gain[None], norm_bias[None], mix_bias)
    tgrad, vout, gout, mout, bout, nout, hout = finish_call(*parts)
    return tgrad[None], vout, gout, mout, bout, nout.reshape(1024), hout.reshape(1024)


def solution(mesh):
    rows = P("dp", "sp", None)
    placed = (rows, rows, rows, rows, P("dp", None), P("dp", None), P(), P(), P(), P())
    return jax.shard_map(
        shards, mesh=mesh, in_specs=placed,
        out_specs=(rows, P("dp", None), P("dp", None), P(), P(), P(), P()), check_vma=False)
```
